512 devices in a mesh: rep: 2 (over z_hi), fs: 32 (over z_lo, y), tp: 8 (over x, core).
Axes of the slice: x: 4, y: 8, z: 8 (z_hi: 2, z_lo: 4; z = z_hi * 4 + z_lo), core: 2. Of those that a mesh axis runs over, the one named last changes fastest.
Arguments:
- tokens: bfloat16 [20480, 2048], P(('rep', 'fs')), may hold values from -6 to 6
- gate_weight: float32 [2048, 5120], P('fs', 'tp'), may hold values from -0.125 to 0.125
- up_weight: float32 [2048, 5120], P('fs', 'tp'), may hold values from -0.125 to 0.125
- down_weight: float32 [2048, 5120], P('fs', 'tp'), may hold values from -0.078125 to 0.078125
- value_weight: float32 [2048, 2048], P('fs', 'tp'), may hold values from -0.125 to 0.125
- glu_weight: float32 [2048, 2048], P('fs', 'tp'), may hold values from -0.125 to 0.125
- out_weight: float32 [2048, 2048], P('fs', 'tp'), may hold values from -0.125 to 0.125
- gate_scale: float32 [5120], P('tp'), may hold values from 0.1 to 1.9
- up_scale: float32 [5120], P('tp'), may hold values from 0.5 to 2
- down_scale: float32 [2048], P('fs'), may hold values from 1 to 4
- value_scale: float32 [2048], P('tp'), may hold values from 0.2 to 3.4
- glu_scale: float32 [2048], P('tp'), may hold values from 0.1 to 1.9
- out_scale: float32 [2048], P('fs'), may hold values from 1 to 4
- conv_kernel: float32 [31, 2048], P(None, 'tp'), may hold values from -1 to 1
- norm_gain: float32 [2048], P('tp'), may hold values from 0.1 to 1.9
- first_gain: float32 [2048], replicated, may hold values from 0.1 to 1.9
- conv_gain: float32 [2048], replicated, may hold values from 0.1 to 1.9
- second_gain: float32 [2048], replicated, may hold values from 0.1 to 1.9
Outputs:
- result: bfloat16 [20480, 2048], P(('rep', 'fs'))
The draws below stay inside these ranges and needn't reach their ends.
All inputs are finite; a program needn't handle non-finite values.
Results may differ from the reference program's by a relative error of at most 0.02.
Values may be sent and summed in bfloat16 or wider, within the bound.
No kernel may reach another device: no remote copies, remote signals or barrier semaphores. Data moves between devices by JAX's collectives and lax.ppermute only.
A program may use at most 64 MiB of HBM per device.

```python
import math
import jax
import jax.numpy as jnp
from jax import lax

D = 2048
FF = 5120
KW = 31
SEQ = 320
TOKENS = 20480
N_REP = 2
N_FS = 32
N_TP = 8


def draw_value_scale(key, part):
    position = jnp.arange(D, dtype=jnp.float32) / D
    noise = jax.random.uniform(key, (D,), jnp.float32, 0.7, 1.4)
    ramp = 0.5 * jnp.exp(jnp.log(4.0) * position)
    return (ramp * noise).astype(jnp.float32)


def shard_levels(rng, shape, pieces, least, high):
    level, own = 1.0, jax.random.fold_in(rng, 6)
    for dim, blocks in pieces:
        draws = jnp.exp(jax.random.uniform(jax.random.fold_in(own, dim), (blocks,), jnp.float32, least / len(pieces), high / len(pieces)))
        level = level * jnp.repeat(draws, shape[dim] // blocks).reshape([-1 if axis == dim else 1 for axis in range(len(shape))])
    return level


def scatter_about(own_key, extent, scale, most, shards=(), kind=jnp.bfloat16):
    array = jax.random.normal(own_key, extent, jnp.float32) * scale
    if len(shards) > 0:
        array = shard_levels(own_key, extent, shards, -0.22, 0.18) * array
    return jnp.clip(array, min=-most, max=most).astype(kind)


def setup_inputs(seed: int = 0) -> dict:
    key_of = jax.random.split(jax.random.key(seed), 19)
    return {
        "tokens": scatter_about(key_of[0], (TOKENS, D), 1.0, 6.0, ((0, 64),)),
        "gate_weight": scatter_about(key_of[1], (D, FF), D ** -0.5, 0.125, ((0, 32), (1, 8)), jnp.float32),
        "up_weight": scatter_about(key_of[2], (D, FF), D ** -0.5, 0.125, ((0, 32), (1, 8)), jnp.float32),
        "down_weight": scatter_about(key_of[3], (D, FF), FF ** -0.5, 0.078125, ((0, 32), (1, 8)), jnp.float32),
        "value_weight": scatter_about(key_of[4], (D, D), D ** -0.5, 0.125, ((0, 32), (1, 8)), jnp.float32),
        "glu_weight": scatter_about(key_of[5], (D, D), D ** -0.5, 0.125, ((0, 32), (1, 8)), jnp.float32),
        "out_weight": scatter_about(key_of[6], (D, D), D ** -0.5, 0.125, ((0, 32), (1, 8)), jnp.float32),
        "gate_scale": jnp.clip(1.0 + 0.18 * jax.random.normal(key_of[7], (FF,), jnp.float32), 0.1, 1.9),
        "up_scale": jnp.clip(jnp.exp(math.log(2.0) - 1.3862944 * jax.random.uniform(key_of[8], (FF,), jnp.float32) ** shard_levels(key_of[8], (FF,), ((0, 8),), -0.2, 0.2)), 0.5, 2.0),
        "down_scale": jnp.clip(jnp.exp(math.log(4.0) - 1.3862944 * jax.random.uniform(key_of[9], (D,), jnp.float32) ** shard_levels(key_of[9], (D,), ((0, 32),), -0.2, 0.2)), 1.0, 4.0),
        "value_scale": draw_value_scale(jax.random.fold_in(key_of[18], 71), 0),
        "glu_scale": jnp.clip(1.0 + 0.18 * jax.random.normal(key_of[11], (D,), jnp.float32), 0.1, 1.9),
        "out_scale": jnp.clip(jnp.exp(math.log(4.0) - 1.3862944 * jax.random.uniform(key_of[12], (D,), jnp.float32) ** shard_levels(key_of[12], (D,), ((0, 32),), -0.2, 0.2)), 1.0, 4.0),
        "conv_kernel": scatter_about(key_of[13], (KW, D), KW ** -0.5, 1.0, ((1, 8),), jnp.float32),
        "norm_gain": jnp.clip(1.0 + 0.18 * jax.random.normal(key_of[14], (D,), jnp.float32), 0.1, 1.9),
        "first_gain": jnp.clip(1.0 + 0.18 * jax.random.normal(key_of[15], (D,), jnp.float32), 0.1, 1.9),
        "conv_gain": jnp.clip(1.0 + 0.18 * jax.random.normal(key_of[16], (D,), jnp.float32), 0.1, 1.9),
        "second_gain": jnp.clip(1.0 + 0.18 * jax.random.normal(key_of[17], (D,), jnp.float32), 0.1, 1.9),
    }


EPSILON = 1e-06

def rms_rows(rows, gains):
    values = rows.astype(jnp.float32)
    scaled = values * lax.rsqrt(lax.optimization_barrier(jnp.mean(values * values, axis=-1, keepdims=True)) + EPSILON)
    return (scaled * gains).astype(jnp.bfloat16)

def gated_hidden(normed, gate_full, up_full, gate_scale, up_scale):
    gate_part = jnp.dot(normed, gate_full, preferred_element_type=jnp.float32) * gate_scale
    upward = jnp.dot(normed, up_full, preferred_element_type=jnp.float32) * up_scale
    return (jax.nn.silu(gate_part) * upward).astype(jnp.bfloat16)

def block_sum(active, weight_rows):
    width = active.shape[1] // N_TP
    total = jnp.zeros((active.shape[0], weight_rows.shape[0]), jnp.float32)
    for block in range(N_TP):
        partial_term = lax.dot_general(active[:, block * width:(block + 1) * width], weight_rows[:, block * width:(block + 1) * width], (((1,), (1,)), ((), ())), preferred_element_type=jnp.float32)
        rounded = lax.optimization_barrier(partial_term.astype(jnp.bfloat16))
        total = total + rounded.astype(jnp.float32)
    return total

def causal_depthwise(inputs, kernel):
    taps = kernel.shape[0]
    length = inputs.shape[0]
    padded = jnp.concatenate([jnp.zeros((taps - 1, inputs.shape[1]), jnp.float32), inputs.astype(jnp.float32)], axis=0)
    total = jnp.zeros((length, inputs.shape[1]), jnp.float32)
    for offset in range(taps):
        total = total + kernel[offset] * padded[offset:offset + length]
    return total

def reference(tokens, gate_weight, up_weight, down_weight, value_weight, glu_weight, out_weight, gate_scale, up_scale, down_scale, value_scale, glu_scale, out_scale, conv_kernel, norm_gain, first_gain, conv_gain, second_gain):
    gate_full = gate_weight.astype(jnp.bfloat16)
    up_full = up_weight.astype(jnp.bfloat16)
    down_full = down_weight.astype(jnp.bfloat16)
    value_full = value_weight.astype(jnp.bfloat16)
    glu_full = glu_weight.astype(jnp.bfloat16)
    out_full = out_weight.astype(jnp.bfloat16)

    def one_sequence(rows):
        hidden = gated_hidden(rms_rows(rows, first_gain), gate_full, up_full, gate_scale, up_scale)
        after_first = (rows.astype(jnp.float32) + 0.5 * down_scale * block_sum(hidden, down_full)).astype(jnp.bfloat16)
        normed = rms_rows(after_first, conv_gain)
        value_part = jnp.dot(normed, value_full, preferred_element_type=jnp.float32) * value_scale
        gate_part = jnp.dot(normed, glu_full, preferred_element_type=jnp.float32) * glu_scale
        glu_in = (value_part * jax.nn.sigmoid(gate_part)).astype(jnp.bfloat16)
        mixed = causal_depthwise(glu_in, conv_kernel)
        mean_rows = lax.optimization_barrier(jnp.mean(mixed, axis=1, keepdims=True))
        square_rows = lax.optimization_barrier(jnp.mean(mixed * mixed, axis=1, keepdims=True))
        normalized = (mixed - mean_rows) * lax.rsqrt(square_rows - mean_rows * mean_rows + EPSILON) * norm_gain
        active = jax.nn.silu(normalized).astype(jnp.bfloat16)
        after_conv = (after_first.astype(jnp.float32) + out_scale * block_sum(active, out_full)).astype(jnp.bfloat16)
        hidden = gated_hidden(rms_rows(after_conv, second_gain), gate_full, up_full, gate_scale, up_scale)
        return (after_conv.astype(jnp.float32) + 0.5 * down_scale * block_sum(hidden, down_full)).astype(jnp.bfloat16)
    groups = tokens.reshape(N_REP * N_FS, SEQ, D)
    return lax.map(one_sequence, groups).reshape(TOKENS, D)
```

```python
import functools
import jax
import jax.numpy as jnp
from jax import lax
from jax.experimental import pallas as pl
from jax.experimental.pallas import tpu as pltpu
from jax.sharding import PartitionSpec as P

D = 2048
EPSILON = 1e-06
RING = 8
CHIPS = 4
ALL = ("rep", "fs", "tp")
BF = jnp.bfloat16


def device_id(ring_z, y, x, core):
    return (ring_z // 4) * 256 + ((ring_z % 4) * 8 + y) * 8 + x * 2 + core


def plane_groups():
    groups = []
    for x in range(CHIPS):
        for p in range(RING):
            groups.append([device_id(z, p, x, 0) for z in range(RING)])
            groups.append([device_id(p, y, x, 1) for y in range(RING)])
    return groups


def plane_shift(step):
    pairs = []
    for x in range(CHIPS):
        for z in range(RING):
            for y in range(RING):
                pairs.append((device_id(z, y, x, 0), device_id(z, (y + step) % RING, x, 0)))
                pairs.append((device_id(z, y, x, 1), device_id((z + step) % RING, y, x, 1)))
    return pairs


def core_swap(value):
    return lax.ppermute(value, "tp", [(i, i ^ 1) for i in range(8)])


def over_x(value):
    groups = [[0, 2, 4, 6], [1, 3, 5, 7]]
    return lax.all_to_all(value, "tp", 0, 0, axis_index_groups=groups, tiled=True)


def place_body(count, fresh, offsets, *refs):
    lines = refs[:count]
    dest, sem = refs[-2], refs[-1]
    copies = []
    at = 0
    for line in lines:
        for j in range(line.shape[0]):
            row = pl.multiple_of(offsets[at], 32)
            copies.append(
                pltpu.make_async_copy(line.at[j], dest.at[pl.ds(row, 32)], sem)
            )
            at += 1
    for copy in copies:
        copy.start()
    for copy in copies:
        copy.wait()


def place(dest, lines, offsets):
    cols = lines[0].shape[-1]
    count = len(lines)
    hbm = pl.BlockSpec(memory_space=pltpu.HBM)
    fresh = dest is None
    operands = list(lines) + ([] if fresh else [dest])
    return pl.pallas_call(
        functools.partial(place_body, count, fresh),
        out_shape=jax.ShapeDtypeStruct((D, cols), BF),
        in_specs=[pl.BlockSpec(memory_space=pltpu.SMEM)] + [hbm] * len(operands),
        out_specs=hbm,
        scratch_shapes=[pltpu.SemaphoreType.DMA],
        input_output_aliases={} if fresh else {1 + count: 0},
    )(offsets, *operands)


def gather_chain(line, line_offsets):
    up, down = plane_shift(1), plane_shift(-1)
    forward, backward = line, line
    dest = None
    for step in range(1, 5):
        if step == 4:
            forward, backward = forward[:4], backward[4:]
        forward = lax.ppermute(forward, ALL, up)
        backward = lax.ppermute(backward, ALL, down)
        low, high = line_offsets(-step), line_offsets(step)
        if step == 1:
            offsets = jnp.concatenate([line_offsets(0), low, high])
            dest = place(None, [line, forward, backward], offsets)
        elif step == 4:
            dest = place(dest, [forward, backward], jnp.concatenate([low[:4], high[4:]]))
        else:
            dest = place(dest, [forward, backward], jnp.concatenate([low, high]))
    return dest


def rms_rows(rows, gains):
    values = rows.astype(jnp.float32)
    scaled = values * lax.rsqrt(jnp.mean(values * values, axis=-1, keepdims=True) + EPSILON)
    return (scaled * gains).astype(BF)


def gated_hidden(normed, gate_full, up_full, gate_scale, up_scale):
    gate_part = jnp.dot(normed, gate_full, preferred_element_type=jnp.float32) * gate_scale
    upward = jnp.dot(normed, up_full, preferred_element_type=jnp.float32) * up_scale
    return (jax.nn.silu(gate_part) * upward).astype(BF)


def causal_depthwise(inputs, kernel):
    taps = kernel.shape[0]
    length = inputs.shape[0]
    padded = jnp.concatenate(
        [jnp.zeros((taps - 1, inputs.shape[1]), jnp.float32), inputs.astype(jnp.float32)], axis=0
    )
    total = jnp.zeros((length, inputs.shape[1]), jnp.float32)
    for offset in range(taps):
        total = total + kernel[offset] * padded[offset : offset + length]
    return total


def project(active, weight_rows):
    return lax.dot_general(
        active, weight_rows, (((1,), (1,)), ((), ())), preferred_element_type=jnp.float32
    ).astype(BF)


def sum_at_owner(own, other):
    pair = (own.astype(jnp.float32) + core_swap(other).astype(jnp.float32)).astype(BF)
    parts = over_x(pair.reshape(CHIPS, -1, D))
    return jnp.sum(parts.astype(jnp.float32), axis=0)


def collect(rows):
    own = over_x(jnp.broadcast_to(rows[None], (CHIPS, *rows.shape))).reshape(-1, D)
    return own, core_swap(own)


def local(
    tokens,
    gate_weight,
    up_weight,
    down_weight,
    value_weight,
    glu_weight,
    out_weight,
    gate_scale,
    up_scale,
    down_scale,
    value_scale,
    glu_scale,
    out_scale,
    conv_kernel,
    norm_gain,
    first_gain,
    conv_gain,
    second_gain,
):
    rep, fs, tp = lax.axis_index("rep"), lax.axis_index("fs"), lax.axis_index("tp")
    core, chip = tp % 2, tp // 2
    ring_z, ring_y = rep * 4 + fs // 8, fs % 8
    first_core = core == 0
    me = jnp.where(first_core, ring_y, ring_z)

    def line_offsets(delta):
        p = jnp.full((RING,), (me + delta + RING) % RING, jnp.int32)
        j = jnp.arange(RING, dtype=jnp.int32)
        z, y = jnp.where(first_core, j, p), jnp.where(first_core, p, j)
        return 64 * (8 * (z % 4) + y) + 32 * (z // 4)

    down_rows = (0.5 * down_scale)[:, None] * down_weight.astype(BF).astype(jnp.float32)
    out_rows = out_scale[:, None] * out_weight.astype(BF).astype(jnp.float32)
    half = rep * 32

    def my_rows(arrays):
        return jnp.concatenate(
            [lax.dynamic_slice_in_dim(a, half, 32, 0).astype(BF) for a in arrays], axis=1
        )

    groups = plane_groups()

    def line_of(block):
        copies = jnp.broadcast_to(block[None], (RING, *block.shape))
        return lax.all_to_all(copies, ALL, 0, 0, axis_index_groups=groups, tiled=True)

    line = line_of(
        my_rows((gate_weight, up_weight, down_rows, value_weight, glu_weight, out_rows))
    )
    ff = gate_weight.shape[1]
    ch = value_weight.shape[1]
    first = gather_chain(line[:, :, : 2 * ff], line_offsets)
    rest = gather_chain(line[:, :, 2 * ff :], line_offsets)
    gate_full, up_full = first[:, :ff], first[:, ff:]
    down_full = rest[:, :ff]
    value_full = rest[:, ff : ff + ch]
    glu_full = rest[:, ff + ch : ff + 2 * ch]
    out_full = rest[:, ff + 2 * ch :]

    rows_half = tokens.shape[0] // 2
    own_count = rows_half // CHIPS
    normed = rms_rows(tokens, first_gain)
    hidden = gated_hidden(normed, gate_full, up_full, gate_scale, up_scale)
    partial = project(hidden, down_full)

    def halves(full):
        own = lax.dynamic_slice_in_dim(full, core * rows_half, rows_half, 0)
        other = lax.dynamic_slice_in_dim(full, (1 - core) * rows_half, rows_half, 0)
        return own, other

    def in_order(own, other):
        return jnp.concatenate(
            [jnp.where(first_core, own, other), jnp.where(first_core, other, own)], axis=0
        )

    own_tokens = lax.dynamic_slice_in_dim(
        tokens, core * rows_half + chip * own_count, own_count, 0
    )
    after_first = (own_tokens.astype(jnp.float32) + sum_at_owner(*halves(partial))).astype(BF)

    def glu_of(rows):
        value_part = jnp.dot(rows, value_full, preferred_element_type=jnp.float32) * value_scale
        gate_part = jnp.dot(rows, glu_full, preferred_element_type=jnp.float32) * glu_scale
        return (value_part * jax.nn.sigmoid(gate_part)).astype(BF)

    own, other = collect(rms_rows(after_first, conv_gain))
    mixed = causal_depthwise(in_order(glu_of(own), glu_of(other)), conv_kernel)
    stats = jnp.stack([jnp.sum(mixed, axis=1), jnp.sum(mixed * mixed, axis=1)])
    stats = lax.all_to_all(jnp.broadcast_to(stats[None], (8, *stats.shape)), "tp", 0, 0, tiled=True)
    stats = jnp.sum(stats, axis=0) / D
    mean_rows, square_rows = stats[0][:, None], stats[1][:, None]
    normalized = (
        (mixed - mean_rows) * lax.rsqrt(square_rows - mean_rows * mean_rows + EPSILON) * norm_gain
    )
    active = jax.nn.silu(normalized).astype(BF)
    after_conv = (
        after_first.astype(jnp.float32) + sum_at_owner(*halves(project(active, out_full)))
    ).astype(BF)

    own, other = collect(rms_rows(after_conv, second_gain))

    def second(rows):
        return project(gated_hidden(rows, gate_full, up_full, gate_scale, up_scale), down_full)

    total = sum_at_owner(second(own), second(other))
    after_second = (after_conv.astype(jnp.float32) + total).astype(BF)
    return in_order(*collect(after_second))


def solution(mesh):
    placed = (
        P(("rep", "fs"), None),
        P("fs", "tp"),
        P("fs", "tp"),
        P("fs", "tp"),
        P("fs", "tp"),
        P("fs", "tp"),
        P("fs", "tp"),
        P("tp"),
        P("tp"),
        P("fs"),
        P("tp"),
        P("tp"),
        P("fs"),
        P(None, "tp"),
        P("tp"),
        P(),
        P(),
        P(),
    )
    return jax.shard_map(
        local, mesh=mesh, in_specs=placed, out_specs=P(("rep", "fs"), None), check_vma=False
    )
```

```python
import functools
import jax
import jax.numpy as jnp
from jax import lax
from jax.experimental import pallas as pl
from jax.experimental.pallas import tpu as pltpu
from jax.sharding import PartitionSpec as P

D = 2048
EPSILON = 1e-06
RING = 8
CHIPS = 4
ALL = ("rep", "fs", "tp")
BF = jnp.bfloat16


def device_id(ring_z, y, x, core):
    return (ring_z // 4) * 256 + ((ring_z % 4) * 8 + y) * 8 + x * 2 + core


def plane_groups():
    groups = []
    for x in range(CHIPS):
        for p in range(RING):
            groups.append([device_id(z, p, x, 0) for z in range(RING)])
            groups.append([device_id(p, y, x, 1) for y in range(RING)])
    return groups


def plane_shift(step):
    pairs = []
    for x in range(CHIPS):
        for z in range(RING):
            for y in range(RING):
                pairs.append((device_id(z, y, x, 0), device_id(z, (y + step) % RING, x, 0)))
                pairs.append((device_id(z, y, x, 1), device_id((z + step) % RING, y, x, 1)))
    return pairs


def core_swap(value):
    return lax.ppermute(value, "tp", [(i, i ^ 1) for i in range(8)])


def over_x(value):
    groups = [[0, 2, 4, 6], [1, 3, 5, 7]]
    return lax.all_to_all(value, "tp", 0, 0, axis_index_groups=groups, tiled=True)


def place_body(count, offsets, *refs):
    lines = refs[:count]
    dest, sem = refs[-2], refs[-1]
    copies = []
    at = 0
    for line in lines:
        for j in range(line.shape[0]):
            row = pl.multiple_of(offsets[at], 32)
            copies.append(pltpu.make_async_copy(line.at[j], dest.at[pl.ds(row, 32)], sem))
            at += 1
    for copy in copies:
        copy.start()
    for copy in copies:
        copy.wait()


def place(lines, offsets):
    cols = lines[0].shape[-1]
    hbm = pl.BlockSpec(memory_space=pltpu.HBM)
    return pl.pallas_call(
        functools.partial(place_body, len(lines)),
        out_shape=jax.ShapeDtypeStruct((D, cols), BF),
        in_specs=[pl.BlockSpec(memory_space=pltpu.SMEM)] + [hbm] * len(lines),
        out_specs=pl.BlockSpec(memory_space=pltpu.VMEM),
        scratch_shapes=[pltpu.SemaphoreType.DMA],
    )(offsets, *lines)


def gather_chain(line, line_offsets):
    up, down = plane_shift(1), plane_shift(-1)
    forward, backward = line, line
    lines, offsets = [line], [line_offsets(0)]
    for step in range(1, 5):
        low, high = line_offsets(-step), line_offsets(step)
        if step == 4:
            forward, backward = forward[:4], backward[4:]
            low, high = low[:4], high[4:]
        forward = lax.ppermute(forward, ALL, up)
        backward = lax.ppermute(backward, ALL, down)
        lines += [forward, backward]
        offsets += [low, high]
    return place(lines, jnp.concatenate(offsets))


def rms_rows(rows, gains):
    values = rows.astype(jnp.float32)
    scaled = values * lax.rsqrt(jnp.mean(values * values, axis=-1, keepdims=True) + EPSILON)
    return (scaled * gains).astype(BF)


def gated_hidden(normed, gate_full, up_full, gate_scale, up_scale):
    gate_part = jnp.dot(normed, gate_full, preferred_element_type=jnp.float32) * gate_scale
    upward = jnp.dot(normed, up_full, preferred_element_type=jnp.float32) * up_scale
    return (jax.nn.silu(gate_part) * upward).astype(BF)


def causal_depthwise(inputs, kernel):
    taps = kernel.shape[0]
    length = inputs.shape[0]
    padded = jnp.concatenate(
        [jnp.zeros((taps - 1, inputs.shape[1]), jnp.float32), inputs.astype(jnp.float32)], axis=0
    )
    total = jnp.zeros((length, inputs.shape[1]), jnp.float32)
    for offset in range(taps):
        total = total + kernel[offset] * padded[offset : offset + length]
    return total


def project(active, weight_rows):
    return lax.dot_general(
        active, weight_rows, (((1,), (1,)), ((), ())), preferred_element_type=jnp.float32
    ).astype(BF)


def sum_at_owner(own, other):
    pair = (own.astype(jnp.float32) + core_swap(other).astype(jnp.float32)).astype(BF)
    parts = over_x(pair.reshape(CHIPS, -1, D))
    return jnp.sum(parts.astype(jnp.float32), axis=0)


def collect(rows):
    own = over_x(jnp.broadcast_to(rows[None], (CHIPS, *rows.shape))).reshape(-1, D)
    return own, core_swap(own)


def local(
    tokens,
    gate_weight,
    up_weight,
    down_weight,
    value_weight,
    glu_weight,
    out_weight,
    gate_scale,
    up_scale,
    down_scale,
    value_scale,
    glu_scale,
    out_scale,
    conv_kernel,
    norm_gain,
    first_gain,
    conv_gain,
    second_gain,
):
    rep, fs, tp = lax.axis_index("rep"), lax.axis_index("fs"), lax.axis_index("tp")
    core, chip = tp % 2, tp // 2
    ring_z, ring_y = rep * 4 + fs // 8, fs % 8
    first_core = core == 0
    me = jnp.where(first_core, ring_y, ring_z)

    def line_offsets(delta):
        p = jnp.full((RING,), (me + delta + RING) % RING, jnp.int32)
        j = jnp.arange(RING, dtype=jnp.int32)
        z, y = jnp.where(first_core, j, p), jnp.where(first_core, p, j)
        return 64 * (8 * (z % 4) + y) + 32 * (z // 4)

    down_rows = (0.5 * down_scale)[:, None] * down_weight.astype(BF).astype(jnp.float32)
    out_rows = out_scale[:, None] * out_weight.astype(BF).astype(jnp.float32)
    half = rep * 32

    def my_rows(arrays):
        return jnp.concatenate(
            [lax.dynamic_slice_in_dim(a, half, 32, 0).astype(BF) for a in arrays], axis=1
        )

    groups = plane_groups()

    def line_of(block):
        copies = jnp.broadcast_to(block[None], (RING, *block.shape))
        return lax.all_to_all(copies, ALL, 0, 0, axis_index_groups=groups, tiled=True)

    line = line_of(
        my_rows((gate_weight, up_weight, down_rows, value_weight, glu_weight, out_rows))
    )
    ff = gate_weight.shape[1]
    ch = value_weight.shape[1]
    first = gather_chain(line[:, :, : 2 * ff], line_offsets)
    rest = gather_chain(line[:, :, 2 * ff :], line_offsets)
    gate_full, up_full = first[:, :ff], first[:, ff:]
    down_full = rest[:, :ff]
    value_full = rest[:, ff : ff + ch]
    glu_full = rest[:, ff + ch : ff + 2 * ch]
    out_full = rest[:, ff + 2 * ch :]

    rows_half = tokens.shape[0] // 2
    own_count = rows_half // CHIPS
    normed = rms_rows(tokens, first_gain)
    hidden = gated_hidden(normed, gate_full, up_full, gate_scale, up_scale)
    partial = project(hidden, down_full)

    def halves(full):
        own = lax.dynamic_slice_in_dim(full, core * rows_half, rows_half, 0)
        other = lax.dynamic_slice_in_dim(full, (1 - core) * rows_half, rows_half, 0)
        return own, other

    def in_order(own, other):
        return jnp.concatenate(
            [jnp.where(first_core, own, other), jnp.where(first_core, other, own)], axis=0
        )

    own_tokens = lax.dynamic_slice_in_dim(
        tokens, core * rows_half + chip * own_count, own_count, 0
    )
    after_first = (own_tokens.astype(jnp.float32) + sum_at_owner(*halves(partial))).astype(BF)

    def glu_of(rows):
        value_part = jnp.dot(rows, value_full, preferred_element_type=jnp.float32) * value_scale
        gate_part = jnp.dot(rows, glu_full, preferred_element_type=jnp.float32) * glu_scale
        return (value_part * jax.nn.sigmoid(gate_part)).astype(BF)

    own, other = collect(rms_rows(after_first, conv_gain))
    mixed = causal_depthwise(in_order(glu_of(own), glu_of(other)), conv_kernel)
    stats = jnp.stack([jnp.sum(mixed, axis=1), jnp.sum(mixed * mixed, axis=1)])
    stats = lax.all_to_all(jnp.broadcast_to(stats[None], (8, *stats.shape)), "tp", 0, 0, tiled=True)
    stats = jnp.sum(stats, axis=0) / D
    mean_rows, square_rows = stats[0][:, None], stats[1][:, None]
    normalized = (
        (mixed - mean_rows) * lax.rsqrt(square_rows - mean_rows * mean_rows + EPSILON) * norm_gain
    )
    active = jax.nn.silu(normalized).astype(BF)
    after_conv = (
        after_first.astype(jnp.float32) + sum_at_owner(*halves(project(active, out_full)))
    ).astype(BF)

    own, other = collect(rms_rows(after_conv, second_gain))

    def second(rows):
        return project(gated_hidden(rows, gate_full, up_full, gate_scale, up_scale), down_full)

    total = sum_at_owner(second(own), second(other))
    after_second = (after_conv.astype(jnp.float32) + total).astype(BF)
    return in_order(*collect(after_second))


def solution(mesh):
    placed = (
        P(("rep", "fs"), None),
        P("fs", "tp"),
        P("fs", "tp"),
        P("fs", "tp"),
        P("fs", "tp"),
        P("fs", "tp"),
        P("fs", "tp"),
        P("tp"),
        P("tp"),
        P("fs"),
        P("tp"),
        P("tp"),
        P("fs"),
        P(None, "tp"),
        P("tp"),
        P(),
        P(),
        P(),
    )
    return jax.shard_map(
        local, mesh=mesh, in_specs=placed, out_specs=P(("rep", "fs"), None), check_vma=False
    )
```

```python
import functools
import jax
import jax.numpy as jnp
from jax import lax
from jax.experimental import pallas as pl
from jax.experimental.pallas import tpu as pltpu
from jax.sharding import PartitionSpec as P

D = 2048
EPSILON = 1e-06
RING = 8
CHIPS = 4
ALL = ("rep", "fs", "tp")
BF = jnp.bfloat16


def device_id(ring_z, y, x, core):
    return (ring_z // 4) * 256 + ((ring_z % 4) * 8 + y) * 8 + x * 2 + core


def plane_groups():
    groups = []
    for x in range(CHIPS):
        for p in range(RING):
            groups.append([device_id(z, p, x, 0) for z in range(RING)])
            groups.append([device_id(p, y, x, 1) for y in range(RING)])
    return groups


def plane_shift(step):
    pairs = []
    for x in range(CHIPS):
        for z in range(RING):
            for y in range(RING):
                pairs.append((device_id(z, y, x, 0), device_id(z, (y + step) % RING, x, 0)))
                pairs.append((device_id(z, y, x, 1), device_id((z + step) % RING, y, x, 1)))
    return pairs


def core_swap(value):
    return lax.ppermute(value, "tp", [(i, i ^ 1) for i in range(8)])


def over_x(value):
    groups = [[0, 2, 4, 6], [1, 3, 5, 7]]
    return lax.all_to_all(value, "tp", 0, 0, axis_index_groups=groups, tiled=True)


def blocks_body(half_ref, gate, up, down, value, glu, out, down_scale, out_scale, first, rest):
    rows = pl.ds(pl.multiple_of(half_ref[0], 32), 32)
    size = down.shape[0]
    diagonal = lax.broadcasted_iota(jnp.int32, (size, size), 0) == lax.broadcasted_iota(
        jnp.int32, (size, size), 1
    )

    def scaled(weight, scale, factor):
        spread = jnp.where(diagonal, jnp.broadcast_to(scale[...], (size, size)), 0.0)
        column = jnp.sum(spread, axis=1, keepdims=True) * factor
        return (weight[...].astype(BF).astype(jnp.float32) * column).astype(BF)

    ff, ch = gate.shape[1], value.shape[1]
    lead = jnp.concatenate([gate[rows, :], up[rows, :]], axis=1).astype(BF)
    kept = half_ref[0] == 0
    down_rows = scaled(down, down_scale, 0.5).astype(jnp.float32)
    out_rows = scaled(out, out_scale, 1.0).astype(jnp.float32)
    tail = jnp.concatenate(
        [
            jnp.where(kept, down_rows[:32], down_rows[32:]),
            value[rows, :],
            glu[rows, :],
            jnp.where(kept, out_rows[:32], out_rows[32:]),
        ],
        axis=1,
    ).astype(BF)
    for j in range(RING):
        first[j] = lead
        rest[j] = tail


def blocks(half, weights, scales):
    ff, ch = weights[0].shape[1], weights[3].shape[1]
    vmem = pl.BlockSpec(memory_space=pltpu.VMEM)
    return pl.pallas_call(
        blocks_body,
        out_shape=(
            jax.ShapeDtypeStruct((RING, 32, 2 * ff), BF),
            jax.ShapeDtypeStruct((RING, 32, ff + 3 * ch), BF),
        ),
        in_specs=[pl.BlockSpec(memory_space=pltpu.SMEM)] + [vmem] * 8,
        out_specs=(vmem, vmem),
        compiler_params=pltpu.CompilerParams(vmem_limit_bytes=24 << 20),
    )(half[None], *weights, *[scale[None, :] for scale in scales])


def place_body(count, offsets, *refs):
    lines = refs[:count]
    dest, sem = refs[-2], refs[-1]
    copies = []
    at = 0
    for line in lines:
        for j in range(line.shape[0]):
            row = pl.multiple_of(offsets[at], 32)
            copies.append(pltpu.make_async_copy(line.at[j], dest.at[pl.ds(row, 32)], sem))
            at += 1
    for copy in copies:
        copy.start()
    for copy in copies:
        copy.wait()


def place(lines, offsets):
    cols = lines[0].shape[-1]
    hbm = pl.BlockSpec(memory_space=pltpu.HBM)
    return pl.pallas_call(
        functools.partial(place_body, len(lines)),
        out_shape=pltpu.VMEM((D, cols), BF),
        in_specs=[pl.BlockSpec(memory_space=pltpu.SMEM)] + [hbm] * len(lines),
        out_specs=pl.BlockSpec(memory_space=pltpu.VMEM),
        scratch_shapes=[pltpu.SemaphoreType.DMA],
        compiler_params=pltpu.CompilerParams(vmem_limit_bytes=1 << 20),
    )(offsets, *lines)


def gather_chain(line, line_offsets):
    up, down = plane_shift(1), plane_shift(-1)
    forward, backward = line, line
    lines, offsets = [line], [line_offsets(0)]
    for step in range(1, 5):
        low, high = line_offsets(-step), line_offsets(step)
        if step == 4:
            forward, backward = forward[:4], backward[4:]
            low, high = low[:4], high[4:]
        forward = lax.ppermute(forward, ALL, up)
        backward = lax.ppermute(backward, ALL, down)
        lines += [forward, backward]
        offsets += [low, high]
    return place(lines, jnp.concatenate(offsets))


def rms_rows(rows, gains):
    values = rows.astype(jnp.float32)
    scaled = values * lax.rsqrt(jnp.mean(values * values, axis=-1, keepdims=True) + EPSILON)
    return (scaled * gains).astype(BF)


def gated_hidden(normed, gate_full, up_full, gate_scale, up_scale):
    gate_part = jnp.dot(normed, gate_full, preferred_element_type=jnp.float32) * gate_scale
    upward = jnp.dot(normed, up_full, preferred_element_type=jnp.float32) * up_scale
    return (jax.nn.silu(gate_part) * upward).astype(BF)


def causal_depthwise(inputs, kernel):
    taps = kernel.shape[0]
    length = inputs.shape[0]
    padded = jnp.concatenate(
        [jnp.zeros((taps - 1, inputs.shape[1]), jnp.float32), inputs.astype(jnp.float32)], axis=0
    )
    total = jnp.zeros((length, inputs.shape[1]), jnp.float32)
    for offset in range(taps):
        total = total + kernel[offset] * padded[offset : offset + length]
    return total


def project(active, weight_rows):
    return lax.dot_general(
        active, weight_rows, (((1,), (1,)), ((), ())), preferred_element_type=jnp.float32
    ).astype(BF)


def sum_at_owner(own, other):
    pair = (own.astype(jnp.float32) + core_swap(other).astype(jnp.float32)).astype(BF)
    parts = over_x(pair.reshape(CHIPS, -1, D))
    return jnp.sum(parts.astype(jnp.float32), axis=0)


def collect(rows):
    own = over_x(jnp.broadcast_to(rows[None], (CHIPS, *rows.shape))).reshape(-1, D)
    return own, core_swap(own)


def local(
    tokens,
    gate_weight,
    up_weight,
    down_weight,
    value_weight,
    glu_weight,
    out_weight,
    gate_scale,
    up_scale,
    down_scale,
    value_scale,
    glu_scale,
    out_scale,
    conv_kernel,
    norm_gain,
    first_gain,
    conv_gain,
    second_gain,
):
    rep, fs, tp = lax.axis_index("rep"), lax.axis_index("fs"), lax.axis_index("tp")
    core, chip = tp % 2, tp // 2
    ring_z, ring_y = rep * 4 + fs // 8, fs % 8
    first_core = core == 0
    me = jnp.where(first_core, ring_y, ring_z)

    def line_offsets(delta):
        p = jnp.full((RING,), (me + delta + RING) % RING, jnp.int32)
        j = jnp.arange(RING, dtype=jnp.int32)
        z, y = jnp.where(first_core, j, p), jnp.where(first_core, p, j)
        return 64 * (8 * (z % 4) + y) + 32 * (z // 4)

    lead, tail = blocks(
        rep * 32,
        (gate_weight, up_weight, down_weight, value_weight, glu_weight, out_weight),
        (down_scale, out_scale),
    )
    groups = plane_groups()

    def line_of(copies):
        return lax.all_to_all(copies, ALL, 0, 0, axis_index_groups=groups, tiled=True)

    ff = gate_weight.shape[1]
    ch = value_weight.shape[1]
    first = gather_chain(line_of(lead), line_offsets)
    rest = gather_chain(line_of(tail), line_offsets)
    gate_full, up_full = first[:, :ff], first[:, ff:]
    down_full = rest[:, :ff]
    value_full = rest[:, ff : ff + ch]
    glu_full = rest[:, ff + ch : ff + 2 * ch]
    out_full = rest[:, ff + 2 * ch :]

    rows_half = tokens.shape[0] // 2
    own_count = rows_half // CHIPS
    normed = rms_rows(tokens, first_gain)
    hidden = gated_hidden(normed, gate_full, up_full, gate_scale, up_scale)
    partial = project(hidden, down_full)

    def halves(full):
        own = lax.dynamic_slice_in_dim(full, core * rows_half, rows_half, 0)
        other = lax.dynamic_slice_in_dim(full, (1 - core) * rows_half, rows_half, 0)
        return own, other

    def in_order(own, other):
        return jnp.concatenate(
            [jnp.where(first_core, own, other), jnp.where(first_core, other, own)], axis=0
        )

    own_tokens = lax.dynamic_slice_in_dim(
        tokens, core * rows_half + chip * own_count, own_count, 0
    )
    after_first = (own_tokens.astype(jnp.float32) + sum_at_owner(*halves(partial))).astype(BF)

    def glu_of(rows):
        value_part = jnp.dot(rows, value_full, preferred_element_type=jnp.float32) * value_scale
        gate_part = jnp.dot(rows, glu_full, preferred_element_type=jnp.float32) * glu_scale
        return (value_part * jax.nn.sigmoid(gate_part)).astype(BF)

    own, other = collect(rms_rows(after_first, conv_gain))
    mixed = causal_depthwise(in_order(glu_of(own), glu_of(other)), conv_kernel)
    stats = jnp.stack([jnp.sum(mixed, axis=1), jnp.sum(mixed * mixed, axis=1)])
    stats = lax.all_to_all(jnp.broadcast_to(stats[None], (8, *stats.shape)), "tp", 0, 0, tiled=True)
    stats = jnp.sum(stats, axis=0) / D
    mean_rows, square_rows = stats[0][:, None], stats[1][:, None]
    normalized = (
        (mixed - mean_rows) * lax.rsqrt(square_rows - mean_rows * mean_rows + EPSILON) * norm_gain
    )
    active = jax.nn.silu(normalized).astype(BF)
    after_conv = (
        after_first.astype(jnp.float32) + sum_at_owner(*halves(project(active, out_full)))
    ).astype(BF)

    own, other = collect(rms_rows(after_conv, second_gain))

    def second(rows):
        return project(gated_hidden(rows, gate_full, up_full, gate_scale, up_scale), down_full)

    total = sum_at_owner(second(own), second(other))
    after_second = (after_conv.astype(jnp.float32) + total).astype(BF)
    return in_order(*collect(after_second))


def solution(mesh):
    placed = (
        P(("rep", "fs"), None),
        P("fs", "tp"),
        P("fs", "tp"),
        P("fs", "tp"),
        P("fs", "tp"),
        P("fs", "tp"),
        P("fs", "tp"),
        P("tp"),
        P("tp"),
        P("fs"),
        P("tp"),
        P("tp"),
        P("fs"),
        P(None, "tp"),
        P("tp"),
        P(),
        P(),
        P(),
    )
    return jax.shard_map(
        local, mesh=mesh, in_specs=placed, out_specs=P(("rep", "fs"), None), check_vma=False
    )
```

```python
import functools
import jax
import jax.numpy as jnp
from jax import lax
from jax.experimental import pallas as pl
from jax.experimental.pallas import tpu as pltpu
from jax.sharding import PartitionSpec as P

D = 2048
EPSILON = 1e-06
RING = 8
CHIPS = 4
ALL = ("rep", "fs", "tp")
BF = jnp.bfloat16


def device_id(ring_z, y, x, core):
    return (ring_z // 4) * 256 + ((ring_z % 4) * 8 + y) * 8 + x * 2 + core


def plane_groups():
    groups = []
    for x in range(CHIPS):
        for p in range(RING):
            groups.append([device_id(z, p, x, 0) for z in range(RING)])
            groups.append([device_id(p, y, x, 1) for y in range(RING)])
    return groups


def plane_shift(step):
    pairs = []
    for x in range(CHIPS):
        for z in range(RING):
            for y in range(RING):
                pairs.append((device_id(z, y, x, 0), device_id(z, (y + step) % RING, x, 0)))
                pairs.append((device_id(z, y, x, 1), device_id((z + step) % RING, y, x, 1)))
    return pairs


def core_swap(value):
    return lax.ppermute(value, "tp", [(i, i ^ 1) for i in range(8)])


def over_x(value):
    groups = [[0, 2, 4, 6], [1, 3, 5, 7]]
    return lax.all_to_all(value, "tp", 0, 0, axis_index_groups=groups, tiled=True)


def blocks_body(half_ref, *refs):
    weights, (down_scale, out_scale, out), bufs, sem = refs[:6], refs[6:9], refs[9:15], refs[15]
    start = pl.multiple_of(half_ref[0], 32)
    copies = [
        pltpu.make_async_copy(w.at[pl.ds(start, 32)], buf, sem.at[k])
        for k, (w, buf) in enumerate(zip(weights, bufs))
    ]
    for copy in copies:
        copy.start()
    shape = (32, 64)
    row = lax.broadcasted_iota(jnp.int32, shape, 0) + half_ref[0]
    diagonal = row == lax.broadcasted_iota(jnp.int32, shape, 1)

    def column(scale, factor):
        spread = jnp.where(diagonal, jnp.broadcast_to(scale[...], shape), 0.0)
        return jnp.sum(spread, axis=1, keepdims=True) * factor

    columns = {2: column(down_scale, 0.5), 5: column(out_scale, 1.0)}
    at = 0
    for k, (copy, buf) in enumerate(zip(copies, bufs)):
        copy.wait()
        value = buf[...].astype(BF)
        if k in columns:
            value = (value.astype(jnp.float32) * columns[k]).astype(BF)
        width = value.shape[1]
        for j in range(RING):
            out[j, :, at : at + width] = value
        at += width


def blocks(half, weights, scales):
    widths = [w.shape[1] for w in weights]
    vmem = pl.BlockSpec(memory_space=pltpu.VMEM)
    hbm = pl.BlockSpec(memory_space=pltpu.HBM)
    return pl.pallas_call(
        blocks_body,
        out_shape=jax.ShapeDtypeStruct((RING, 32, sum(widths)), BF),
        in_specs=[pl.BlockSpec(memory_space=pltpu.SMEM)] + [hbm] * 6 + [vmem] * 2,
        out_specs=vmem,
        scratch_shapes=[pltpu.VMEM((32, w), jnp.float32) for w in widths]
        + [pltpu.SemaphoreType.DMA((6,))],
    )(half[None], *weights, *[scale[None, :] for scale in scales])


def gather_chain(line):
    up, down = plane_shift(1), plane_shift(-1)
    forward, backward = line, line
    lines = [line]
    for step in range(1, 5):
        if step == 4:
            forward, backward = forward[:4], backward[4:]
        forward = lax.ppermute(forward, ALL, up)
        backward = lax.ppermute(backward, ALL, down)
        lines += [forward, backward]
    return lines


DELTAS = (0, -1, 1, -2, 2, -3, 3, -4, 4)


def silu(value):
    return value / (1.0 + jnp.exp(-value))


def matrix(ref, columns):
    value = ref[:, :, :, :, columns]
    return value.reshape(D, value.shape[-1])


def gated(normed, wide, gate_scale, up_scale):
    ff = gate_scale.shape[1]
    gate_part = jnp.dot(
        normed, matrix(wide, slice(0, ff)), preferred_element_type=jnp.float32
    ) * gate_scale[...]
    upward = jnp.dot(
        normed, matrix(wide, slice(ff, 2 * ff)), preferred_element_type=jnp.float32
    ) * up_scale[...]
    return (silu(gate_part) * upward).astype(BF)


def across(active, weight):
    return lax.dot_general(
        active, weight, (((1,), (1,)), ((), ())), preferred_element_type=jnp.float32
    ).astype(BF)


def normalize(rows, gain):
    values = rows.astype(jnp.float32)
    scaled = values * lax.rsqrt(jnp.mean(values * values, axis=-1, keepdims=True) + EPSILON)
    return (scaled * gain).astype(BF)


def line_copies(core, places, source, columns, dest, sem):
    copies = []
    for index, line in enumerate(source):
        p = places[index]
        for h in range(line.shape[0] // 4):
            half = h if line.shape[0] == 8 else (0 if index == 7 else 1)
            part = line.at[pl.ds(4 * h, 4), :, columns]
            copies.append(
                (
                    pltpu.make_async_copy(part, dest.at[:, p, half], sem),
                    pltpu.make_async_copy(part, dest.at[p % 4, pl.ds(4 * half, 4), p // 4], sem),
                )
            )
    return copies


def entry_body(scalars, *refs):
    first, rest = refs[:9], refs[9:18]
    tokens, gain, gate_scale, up_scale = refs[18:22]
    other, own_hidden, wide_out, down_out, conv_out = refs[22:27]
    wide, down, conv, hidden, sems = refs[27:]
    core = scalars[0]
    places = [scalars[1 + k] for k in range(9)]
    ff = gate_scale.shape[1]
    channels = conv.shape[-1]
    groups = [
        line_copies(core, places, first, slice(0, 2 * ff), wide, sems.at[0]),
        line_copies(core, places, rest, slice(0, ff), down, sems.at[1]),
        line_copies(core, places, rest, slice(ff, ff + channels), conv, sems.at[2]),
    ]

    @pl.when(core == 0)
    def _():
        for group in groups:
            for copy, _ in group:
                copy.start()

    @pl.when(core == 1)
    def _():
        for group in groups:
            for _, copy in group:
                copy.start()

    stores = [
        pltpu.make_async_copy(src, dst, sems.at[3 + k])
        for k, (src, dst) in enumerate(((wide, wide_out), (down, down_out), (conv, conv_out)))
    ]
    normed = normalize(tokens[...], gain[...])
    for copy, _ in groups[0]:
        copy.wait()
    stores[0].start()
    hidden[...] = gated(normed, wide, gate_scale, up_scale)
    for copy, _ in groups[1]:
        copy.wait()
    stores[1].start()
    for copy, _ in groups[2]:
        copy.wait()
    stores[2].start()
    count = other.shape[0]
    own_at = pl.multiple_of(core * count, count)
    other_at = pl.multiple_of((1 - core) * count, count)
    own_hidden[...] = hidden[pl.ds(own_at, count)]
    other[...] = across(hidden[pl.ds(other_at, count)], matrix(down, slice(None)))
    for store in stores:
        store.wait()


def entry(scalars, first, rest, tokens, gain, gate_scale, up_scale):
    rows = tokens.shape[0]
    ff = gate_scale.shape[0]
    channels = rest[0].shape[-1] - ff
    smem = pl.BlockSpec(memory_space=pltpu.SMEM)
    hbm = pl.BlockSpec(memory_space=pltpu.HBM)
    vmem = pl.BlockSpec(memory_space=pltpu.VMEM)
    grid_shape = (4, 8, 2, 32)
    shapes = [(*grid_shape, 2 * ff), (*grid_shape, ff), (*grid_shape, channels)]
    return pl.pallas_call(
        entry_body,
        out_shape=(
            jax.ShapeDtypeStruct((rows // 2, D), BF),
            jax.ShapeDtypeStruct((rows // 2, ff), BF),
            *[jax.ShapeDtypeStruct(shape, BF) for shape in shapes],
        ),
        in_specs=[smem] + [hbm] * 18 + [vmem] * 4,
        out_specs=(vmem, vmem, hbm, hbm, hbm),
        scratch_shapes=[pltpu.VMEM(shape, BF) for shape in shapes]
        + [pltpu.VMEM((rows, ff), BF), pltpu.SemaphoreType.DMA((6,))],
        cost_estimate=pl.CostEstimate(
            flops=2 * rows * D * 3 * ff, bytes_accessed=24 << 20, transcendentals=rows * ff
        ),
    )(scalars, *first, *rest, tokens, gain[None, :], gate_scale[None, :], up_scale[None, :])


def hidden_body(own, other, wide, down, gate_scale, up_scale, sent, own_hidden):
    own_hidden[...] = gated(own[...], wide, gate_scale, up_scale)
    late = gated(other[...], wide, gate_scale, up_scale)
    sent[...] = across(late, matrix(down, slice(None)))


def again(own, other, wide, down, gate_scale, up_scale):
    rows, ff = own.shape[0], gate_scale.shape[0]
    vmem = pl.BlockSpec(memory_space=pltpu.VMEM)
    return pl.pallas_call(
        hidden_body,
        out_shape=(
            jax.ShapeDtypeStruct((rows, D), BF),
            jax.ShapeDtypeStruct((rows, ff), BF),
        ),
        in_specs=[vmem] * 6,
        out_specs=(vmem, vmem),
        cost_estimate=pl.CostEstimate(
            flops=2 * rows * D * 5 * ff, bytes_accessed=10 << 20, transcendentals=2 * rows * ff
        ),
    )(own, other, wide, down, gate_scale[None, :], up_scale[None, :])


def kept_body(hidden, down, out):
    out[...] = across(hidden[...], matrix(down, slice(None)))


def kept(hidden, down):
    vmem = pl.BlockSpec(memory_space=pltpu.VMEM)
    rows, ff = hidden.shape
    return pl.pallas_call(
        kept_body,
        out_shape=jax.ShapeDtypeStruct((rows, D), BF),
        in_specs=[vmem] * 2,
        out_specs=vmem,
        cost_estimate=pl.CostEstimate(
            flops=2 * rows * D * ff, bytes_accessed=4 << 20, transcendentals=0
        ),
    )(hidden, down)


def rms_rows(rows, gains):
    values = rows.astype(jnp.float32)
    scaled = values * lax.rsqrt(jnp.mean(values * values, axis=-1, keepdims=True) + EPSILON)
    return (scaled * gains).astype(BF)


def causal_depthwise(inputs, kernel):
    taps = kernel.shape[0]
    length = inputs.shape[0]
    padded = jnp.concatenate(
        [jnp.zeros((taps - 1, inputs.shape[1]), jnp.float32), inputs.astype(jnp.float32)], axis=0
    )
    total = jnp.zeros((length, inputs.shape[1]), jnp.float32)
    for offset in range(taps):
        total = total + kernel[offset] * padded[offset : offset + length]
    return total


def project(active, weight_rows):
    return lax.dot_general(
        active, weight_rows, (((1,), (1,)), ((), ())), preferred_element_type=jnp.float32
    ).astype(BF)


def sum_at_owner(own, other):
    pair = (own.astype(jnp.float32) + core_swap(other).astype(jnp.float32)).astype(BF)
    parts = over_x(pair.reshape(CHIPS, -1, D))
    return jnp.sum(parts.astype(jnp.float32), axis=0)


def collect(rows):
    own = over_x(jnp.broadcast_to(rows[None], (CHIPS, *rows.shape))).reshape(-1, D)
    return own, core_swap(own)


def local(
    tokens,
    gate_weight,
    up_weight,
    down_weight,
    value_weight,
    glu_weight,
    out_weight,
    gate_scale,
    up_scale,
    down_scale,
    value_scale,
    glu_scale,
    out_scale,
    conv_kernel,
    norm_gain,
    first_gain,
    conv_gain,
    second_gain,
):
    rep, fs, tp = lax.axis_index("rep"), lax.axis_index("fs"), lax.axis_index("tp")
    core, chip = tp % 2, tp // 2
    ring_z, ring_y = rep * 4 + fs // 8, fs % 8
    first_core = core == 0
    me = jnp.where(first_core, ring_y, ring_z)

    scalars = jnp.stack([core] + [(me + delta + RING) % RING for delta in DELTAS])
    block = blocks(
        rep * 32,
        (gate_weight, up_weight, down_weight, value_weight, glu_weight, out_weight),
        (down_scale, out_scale),
    )
    line = lax.all_to_all(block, ALL, 0, 0, axis_index_groups=plane_groups(), tiled=True)
    ff = gate_weight.shape[1]
    ch = value_weight.shape[1]
    first = gather_chain(line[:, :, : 2 * ff])
    rest = gather_chain(line[:, :, 2 * ff :])
    rows_half = tokens.shape[0] // 2
    own_count = rows_half // CHIPS
    sent, own_hidden, wide, down, conv = entry(
        scalars, first, rest, tokens, first_gain, gate_scale, up_scale
    )
    conv = conv.reshape(D, 3 * ch)
    value_full, glu_full, out_full = conv[:, :ch], conv[:, ch : 2 * ch], conv[:, 2 * ch :]

    def halves(full):
        own = lax.dynamic_slice_in_dim(full, core * rows_half, rows_half, 0)
        other = lax.dynamic_slice_in_dim(full, (1 - core) * rows_half, rows_half, 0)
        return own, other

    def in_order(own, other):
        return jnp.concatenate(
            [jnp.where(first_core, own, other), jnp.where(first_core, other, own)], axis=0
        )

    own_tokens = lax.dynamic_slice_in_dim(
        tokens, core * rows_half + chip * own_count, own_count, 0
    )
    after_first = (own_tokens.astype(jnp.float32) + sum_at_owner(kept(own_hidden, down), sent)).astype(BF)

    def glu_of(rows):
        value_part = jnp.dot(rows, value_full, preferred_element_type=jnp.float32) * value_scale
        gate_part = jnp.dot(rows, glu_full, preferred_element_type=jnp.float32) * glu_scale
        return (value_part * jax.nn.sigmoid(gate_part)).astype(BF)

    own, other = collect(rms_rows(after_first, conv_gain))
    mixed = causal_depthwise(in_order(glu_of(own), glu_of(other)), conv_kernel)
    stats = jnp.stack([jnp.sum(mixed, axis=1), jnp.sum(mixed * mixed, axis=1)])
    stats = lax.all_to_all(jnp.broadcast_to(stats[None], (8, *stats.shape)), "tp", 0, 0, tiled=True)
    stats = jnp.sum(stats, axis=0) / D
    mean_rows, square_rows = stats[0][:, None], stats[1][:, None]
    normalized = (
        (mixed - mean_rows) * lax.rsqrt(square_rows - mean_rows * mean_rows + EPSILON) * norm_gain
    )
    active = jax.nn.silu(normalized).astype(BF)
    after_conv = (
        after_first.astype(jnp.float32) + sum_at_owner(*halves(project(active, out_full)))
    ).astype(BF)

    own, other = collect(rms_rows(after_conv, second_gain))

    sent, own_hidden = again(own, other, wide, down, gate_scale, up_scale)
    total = sum_at_owner(kept(own_hidden, down), sent)
    after_second = (after_conv.astype(jnp.float32) + total).astype(BF)
    return in_order(*collect(after_second))


def solution(mesh):
    placed = (
        P(("rep", "fs"), None),
        P("fs", "tp"),
        P("fs", "tp"),
        P("fs", "tp"),
        P("fs", "tp"),
        P("fs", "tp"),
        P("fs", "tp"),
        P("tp"),
        P("tp"),
        P("fs"),
        P("tp"),
        P("tp"),
        P("fs"),
        P(None, "tp"),
        P("tp"),
        P(),
        P(),
        P(),
    )
    return jax.shard_map(
        local, mesh=mesh, in_specs=placed, out_specs=P(("rep", "fs"), None), check_vma=False
    )
```

```python
import functools
import jax
import jax.numpy as jnp
from jax import lax
from jax.experimental import pallas as pl
from jax.experimental.pallas import tpu as pltpu
from jax.sharding import PartitionSpec as P

D = 2048
EPSILON = 1e-06
RING = 8
CHIPS = 4
ALL = ("rep", "fs", "tp")
BF = jnp.bfloat16


def device_id(ring_z, y, x, core):
    return (ring_z // 4) * 256 + ((ring_z % 4) * 8 + y) * 8 + x * 2 + core


def plane_groups():
    groups = []
    for x in range(CHIPS):
        for p in range(RING):
            groups.append([device_id(z, p, x, 0) for z in range(RING)])
            groups.append([device_id(p, y, x, 1) for y in range(RING)])
    return groups


def plane_shift(step):
    pairs = []
    for x in range(CHIPS):
        for z in range(RING):
            for y in range(RING):
                pairs.append((device_id(z, y, x, 0), device_id(z, (y + step) % RING, x, 0)))
                pairs.append((device_id(z, y, x, 1), device_id((z + step) % RING, y, x, 1)))
    return pairs


def core_swap(value):
    return lax.ppermute(value, "tp", [(i, i ^ 1) for i in range(8)])


def blocks_body(half_ref, *refs):
    weights, (down_scale, out_scale, out), bufs, sem = refs[:6], refs[6:9], refs[9:15], refs[15]
    start = pl.multiple_of(half_ref[0], 32)
    copies = [
        pltpu.make_async_copy(w.at[pl.ds(start, 32)], buf, sem.at[k])
        for k, (w, buf) in enumerate(zip(weights, bufs))
    ]
    for copy in copies:
        copy.start()
    shape = (32, 64)
    row = lax.broadcasted_iota(jnp.int32, shape, 0) + half_ref[0]
    diagonal = row == lax.broadcasted_iota(jnp.int32, shape, 1)

    def column(scale, factor):
        spread = jnp.where(diagonal, jnp.broadcast_to(scale[...], shape), 0.0)
        return jnp.sum(spread, axis=1, keepdims=True) * factor

    columns = {2: column(down_scale, 0.5), 5: column(out_scale, 1.0)}
    at = 0
    for k, (copy, buf) in enumerate(zip(copies, bufs)):
        copy.wait()
        value = buf[...].astype(BF)
        if k in columns:
            value = (value.astype(jnp.float32) * columns[k]).astype(BF)
        width = value.shape[1]
        for j in range(RING):
            out[j, :, at : at + width] = value
        at += width


def blocks(half, weights, scales):
    widths = [w.shape[1] for w in weights]
    vmem = pl.BlockSpec(memory_space=pltpu.VMEM)
    hbm = pl.BlockSpec(memory_space=pltpu.HBM)
    return pl.pallas_call(
        blocks_body,
        out_shape=jax.ShapeDtypeStruct((RING, 32, sum(widths)), BF),
        in_specs=[pl.BlockSpec(memory_space=pltpu.SMEM)] + [hbm] * 6 + [vmem] * 2,
        out_specs=vmem,
        scratch_shapes=[pltpu.VMEM((32, w), jnp.float32) for w in widths]
        + [pltpu.SemaphoreType.DMA((6,))],
    )(half[None], *weights, *[scale[None, :] for scale in scales])


def gather_chain(line):
    up, down = plane_shift(1), plane_shift(-1)
    forward, backward = line, line
    lines = [line]
    for step in range(1, 5):
        if step == 4:
            forward, backward = forward[:4], backward[4:]
        forward = lax.ppermute(forward, ALL, up)
        backward = lax.ppermute(backward, ALL, down)
        lines += [forward, backward]
    return lines


DELTAS = (0, -1, 1, -2, 2, -3, 3, -4, 4)


def silu(value):
    return value / (1.0 + jnp.exp(-value))


def matrix(ref, columns):
    value = ref[:, :, :, :, columns]
    return value.reshape(D, value.shape[-1])


def gated(normed, wide, gate_scale, up_scale):
    ff = gate_scale.shape[1]
    gate_part = jnp.dot(
        normed, matrix(wide, slice(0, ff)), preferred_element_type=jnp.float32
    ) * gate_scale[...]
    upward = jnp.dot(
        normed, matrix(wide, slice(ff, 2 * ff)), preferred_element_type=jnp.float32
    ) * up_scale[...]
    return (silu(gate_part) * upward).astype(BF)


def across(active, weight):
    return lax.dot_general(
        active, weight, (((1,), (1,)), ((), ())), preferred_element_type=jnp.float32
    ).astype(BF)


def normalize(rows, gain):
    values = rows.astype(jnp.float32)
    scaled = values * lax.rsqrt(jnp.mean(values * values, axis=-1, keepdims=True) + EPSILON)
    return (scaled * gain).astype(BF)


def line_copies(places, source, columns, dest, sem):
    copies = []
    for index, line in enumerate(source):
        p = places[index]
        for h in range(line.shape[0] // 4):
            half = h if line.shape[0] == 8 else (0 if index == 7 else 1)
            part = line.at[pl.ds(4 * h, 4), :, columns]
            copies.append(
                (
                    pltpu.make_async_copy(part, dest.at[:, p, half], sem),
                    pltpu.make_async_copy(part, dest.at[p % 4, pl.ds(4 * half, 4), p // 4], sem),
                )
            )
    return copies


def start_lines(core, groups):
    for which in range(2):

        @pl.when(core == which)
        def _():
            for group in groups:
                for pair in group:
                    pair[which].start()


def wait_lines(group):
    for copy, _ in group:
        copy.wait()


def own_and_other(core, count):
    own = pl.ds(pl.multiple_of(core * count, count), count)
    other = pl.ds(pl.multiple_of((1 - core) * count, count), count)
    return own, other


def entry_body(scalars, *refs):
    first, rest = refs[:9], refs[9:18]
    tokens, gain, gate_scale, up_scale = refs[18:22]
    sent, kept, wide_out, down_out = refs[22:26]
    wide, down, normed, sems = refs[26:]
    core = scalars[0]
    places = [scalars[1 + k] for k in range(9)]
    ff = gate_scale.shape[1]
    everything = slice(None)
    wide_lines = line_copies(places, first, everything, wide, sems.at[0])
    down_lines = line_copies(places, rest, slice(0, ff), down, sems.at[1])
    start_lines(core, (wide_lines, down_lines))
    stores = [
        pltpu.make_async_copy(wide, wide_out, sems.at[2]),
        pltpu.make_async_copy(down, down_out, sems.at[3]),
    ]
    count = sent.shape[0]
    for at, rows in zip((0, count), own_and_other(core, count)):
        normed[at : at + count] = normalize(tokens[rows, :], gain[...])
    wait_lines(wide_lines)
    stores[0].start()
    hidden = gated(normed[...], wide, gate_scale, up_scale)
    wait_lines(down_lines)
    stores[1].start()
    partial = across(hidden, matrix(down, everything))
    kept[...] = partial[:count]
    sent[...] = partial[count:]
    for store in stores:
        store.wait()


def entry(scalars, first, rest, tokens, gain, gate_scale, up_scale):
    rows = tokens.shape[0]
    ff = gate_scale.shape[0]
    smem = pl.BlockSpec(memory_space=pltpu.SMEM)
    hbm = pl.BlockSpec(memory_space=pltpu.HBM)
    vmem = pl.BlockSpec(memory_space=pltpu.VMEM)
    shapes = [(4, 8, 2, 32, 2 * ff), (4, 8, 2, 32, ff)]
    half = jax.ShapeDtypeStruct((rows // 2, D), BF)
    return pl.pallas_call(
        entry_body,
        out_shape=(half, half, *[jax.ShapeDtypeStruct(shape, BF) for shape in shapes]),
        in_specs=[smem] + [hbm] * 18 + [vmem] * 4,
        out_specs=(vmem, vmem, hbm, hbm),
        scratch_shapes=[pltpu.VMEM(shape, BF) for shape in shapes]
        + [pltpu.VMEM((rows, D), BF), pltpu.SemaphoreType.DMA((4,))],
        cost_estimate=pl.CostEstimate(
            flops=2 * rows * D * 3 * ff, bytes_accessed=16 << 20, transcendentals=rows * ff
        ),
    )(scalars, *first, *rest, tokens, gain[None, :], gate_scale[None, :], up_scale[None, :])


def again_body(own, other, wide, down, gate_scale, up_scale, sent, kept):
    rows = jnp.concatenate([own[...], other[...]], axis=0)
    hidden = gated(rows, wide, gate_scale, up_scale)
    partial = across(hidden, matrix(down, slice(None)))
    count = own.shape[0]
    kept[...] = partial[:count]
    sent[...] = partial[count:]


def again(own, other, wide, down, gate_scale, up_scale):
    rows, ff = own.shape[0], gate_scale.shape[0]
    vmem = pl.BlockSpec(memory_space=pltpu.VMEM)
    half = jax.ShapeDtypeStruct((rows, D), BF)
    return pl.pallas_call(
        again_body,
        out_shape=(half, half),
        in_specs=[vmem] * 6,
        out_specs=(vmem, vmem),
        cost_estimate=pl.CostEstimate(
            flops=2 * rows * D * 6 * ff, bytes_accessed=10 << 20, transcendentals=2 * rows * ff
        ),
    )(own, other, wide, down, gate_scale[None, :], up_scale[None, :])


def glu_body(scalars, *refs):
    lines = refs[:9]
    own, other, value_scale, glu_scale = refs[9:13]
    glu_in, out_rows = refs[13:15]
    pair, tail, sems = refs[15:]
    core = scalars[0]
    places = [scalars[1 + k] for k in range(9)]
    ch = value_scale.shape[1]
    at = lines[0].shape[-1] - 3 * ch
    pair_lines = line_copies(places, lines, slice(at, at + 2 * ch), pair, sems.at[0])
    tail_lines = line_copies(places, lines, slice(at + 2 * ch, at + 3 * ch), tail, sems.at[1])
    start_lines(core, (pair_lines, tail_lines))
    rows = jnp.concatenate([own[...], other[...]], axis=0)
    wait_lines(pair_lines)
    value_part = jnp.dot(
        rows, matrix(pair, slice(0, ch)), preferred_element_type=jnp.float32
    ) * value_scale[...]
    gate_part = jnp.dot(
        rows, matrix(pair, slice(ch, 2 * ch)), preferred_element_type=jnp.float32
    ) * glu_scale[...]
    result = (value_part / (1.0 + jnp.exp(-gate_part))).astype(BF)
    count = own.shape[0]
    own_rows, other_rows = own_and_other(core, count)
    glu_in[own_rows, :] = result[:count]
    glu_in[other_rows, :] = result[count:]
    wait_lines(tail_lines)
    out_rows[...] = matrix(tail, slice(None))


def glu_of(scalars, lines, own, other, value_scale, glu_scale):
    rows, ch = own.shape[0], value_scale.shape[0]
    smem = pl.BlockSpec(memory_space=pltpu.SMEM)
    hbm = pl.BlockSpec(memory_space=pltpu.HBM)
    vmem = pl.BlockSpec(memory_space=pltpu.VMEM)
    return pl.pallas_call(
        glu_body,
        out_shape=(
            jax.ShapeDtypeStruct((2 * rows, ch), BF),
            jax.ShapeDtypeStruct((D, ch), BF),
        ),
        in_specs=[smem] + [hbm] * 9 + [vmem] * 4,
        out_specs=(vmem, vmem),
        scratch_shapes=[
            pltpu.VMEM((4, 8, 2, 32, 2 * ch), BF),
            pltpu.VMEM((4, 8, 2, 32, ch), BF),
            pltpu.SemaphoreType.DMA((2,)),
        ],
        cost_estimate=pl.CostEstimate(
            flops=2 * rows * D * 4 * ch, bytes_accessed=6 << 20, transcendentals=2 * rows * ch
        ),
    )(scalars, *lines, own, other, value_scale[None, :], glu_scale[None, :])


def causal_depthwise(inputs, kernel):
    taps = kernel.shape[0]
    length = inputs.shape[0]
    padded = jnp.concatenate(
        [jnp.zeros((taps - 1, inputs.shape[1]), jnp.float32), inputs.astype(jnp.float32)], axis=0
    )
    total = jnp.zeros((length, inputs.shape[1]), jnp.float32)
    for offset in range(taps):
        total = total + kernel[offset] * padded[offset : offset + length]
    return total


def project(active, weight_rows):
    return lax.dot_general(
        active, weight_rows, (((1,), (1,)), ((), ())), preferred_element_type=jnp.float32
    ).astype(BF)


def finish_body(pair, right, opposite, left, residual, *refs):
    total = (pair[...].astype(jnp.float32) + opposite[...].astype(jnp.float32)) + (
        left[...].astype(jnp.float32) + right[...].astype(jnp.float32)
    )
    result = (residual[...].astype(jnp.float32) + total).astype(BF)
    if len(refs) == 1:
        refs[0][...] = result
    else:
        gain, out, normed = refs
        out[...] = result
        normed[...] = normalize(result, gain[...])


def finish(mine, sent, residual, gain=None):
    pair = (mine.astype(jnp.float32) + core_swap(sent).astype(jnp.float32)).astype(BF)
    moved = [
        lax.ppermute(pair, "tp", [(i, (i + 2 * hop) % 8) for i in range(8)]) for hop in (1, 2, 3)
    ]
    vmem = pl.BlockSpec(memory_space=pltpu.VMEM)
    shape = jax.ShapeDtypeStruct(pair.shape, BF)
    outs = 1 if gain is None else 2
    extra = [] if gain is None else [gain[None, :]]
    return pl.pallas_call(
        finish_body,
        out_shape=(shape,) * outs,
        in_specs=[vmem] * (5 + len(extra)),
        out_specs=(vmem,) * outs,
    )(pair, *moved, residual, *extra)


def local(
    tokens,
    gate_weight,
    up_weight,
    down_weight,
    value_weight,
    glu_weight,
    out_weight,
    gate_scale,
    up_scale,
    down_scale,
    value_scale,
    glu_scale,
    out_scale,
    conv_kernel,
    norm_gain,
    first_gain,
    conv_gain,
    second_gain,
):
    rep, fs, tp = lax.axis_index("rep"), lax.axis_index("fs"), lax.axis_index("tp")
    core = tp % 2
    ring_z, ring_y = rep * 4 + fs // 8, fs % 8
    first_core = core == 0
    me = jnp.where(first_core, ring_y, ring_z)

    scalars = jnp.stack([core] + [(me + delta + RING) % RING for delta in DELTAS])
    block = blocks(
        rep * 32,
        (gate_weight, up_weight, down_weight, value_weight, glu_weight, out_weight),
        (down_scale, out_scale),
    )
    line = lax.all_to_all(block, ALL, 0, 0, axis_index_groups=plane_groups(), tiled=True)
    ff = gate_weight.shape[1]
    ch = value_weight.shape[1]
    first = gather_chain(line[:, :, : 2 * ff])
    rest = gather_chain(line[:, :, 2 * ff :])
    rows_half = tokens.shape[0] // 2
    sent, mine, wide, down = entry(scalars, first, rest, tokens, first_gain, gate_scale, up_scale)

    def halves(full):
        own = lax.dynamic_slice_in_dim(full, core * rows_half, rows_half, 0)
        other = lax.dynamic_slice_in_dim(full, (1 - core) * rows_half, rows_half, 0)
        return own, other

    def in_order(own, other):
        return jnp.concatenate(
            [jnp.where(first_core, own, other), jnp.where(first_core, other, own)], axis=0
        )

    own_tokens = lax.dynamic_slice_in_dim(tokens, core * rows_half, rows_half, 0)
    after_first, own = finish(mine, sent, own_tokens, conv_gain)
    other = core_swap(own)
    glu_in, out_full = glu_of(scalars, rest, own, other, value_scale, glu_scale)
    mixed = causal_depthwise(glu_in, conv_kernel)
    stats = jnp.stack([jnp.sum(mixed, axis=1), jnp.sum(mixed * mixed, axis=1)])
    stats = lax.all_to_all(jnp.broadcast_to(stats[None], (8, *stats.shape)), "tp", 0, 0, tiled=True)
    stats = jnp.sum(stats, axis=0) / D
    mean_rows, square_rows = stats[0][:, None], stats[1][:, None]
    normalized = (
        (mixed - mean_rows) * lax.rsqrt(square_rows - mean_rows * mean_rows + EPSILON) * norm_gain
    )
    active = jax.nn.silu(normalized).astype(BF)
    mine, sent = halves(project(active, out_full))
    after_conv, own = finish(mine, sent, after_first, second_gain)
    other = core_swap(own)
    sent, mine = again(own, other, wide, down, gate_scale, up_scale)
    (own,) = finish(mine, sent, after_conv)
    return in_order(own, core_swap(own))


def solution(mesh):
    placed = (
        P(("rep", "fs"), None),
        P("fs", "tp"),
        P("fs", "tp"),
        P("fs", "tp"),
        P("fs", "tp"),
        P("fs", "tp"),
        P("fs", "tp"),
        P("tp"),
        P("tp"),
        P("fs"),
        P("tp"),
        P("tp"),
        P("fs"),
        P(None, "tp"),
        P("tp"),
        P(),
        P(),
        P(),
    )
    return jax.shard_map(
        local, mesh=mesh, in_specs=placed, out_specs=P(("rep", "fs"), None), check_vma=False
    )
```

```python
import functools
import jax
import jax.numpy as jnp
from jax import lax
from jax.experimental import pallas as pl
from jax.experimental.pallas import tpu as pltpu
from jax.sharding import PartitionSpec as P

D = 2048
EPSILON = 1e-06
RING = 8
CHIPS = 4
ALL = ("rep", "fs", "tp")
BF = jnp.bfloat16


def device_id(ring_z, y, x, core):
    return (ring_z // 4) * 256 + ((ring_z % 4) * 8 + y) * 8 + x * 2 + core


def plane_groups():
    groups = []
    for x in range(CHIPS):
        for p in range(RING):
            groups.append([device_id(z, p, x, 0) for z in range(RING)])
            groups.append([device_id(p, y, x, 1) for y in range(RING)])
    return groups


def plane_shift(step):
    pairs = []
    for x in range(CHIPS):
        for z in range(RING):
            for y in range(RING):
                pairs.append((device_id(z, y, x, 0), device_id(z, (y + step) % RING, x, 0)))
                pairs.append((device_id(z, y, x, 1), device_id((z + step) % RING, y, x, 1)))
    return pairs


def core_swap(value):
    return lax.ppermute(value, "tp", [(i, i ^ 1) for i in range(8)])


def over_x(value):
    groups = [[0, 2, 4, 6], [1, 3, 5, 7]]
    return lax.all_to_all(value, "tp", 0, 0, axis_index_groups=groups, tiled=True)


def blocks_body(half_ref, *refs):
    weights, (down_scale, out_scale, out), bufs, sem = refs[:6], refs[6:9], refs[9:15], refs[15]
    start = pl.multiple_of(half_ref[0], 32)
    copies = [
        pltpu.make_async_copy(w.at[pl.ds(start, 32)], buf, sem.at[k])
        for k, (w, buf) in enumerate(zip(weights, bufs))
    ]
    for copy in copies:
        copy.start()
    shape = (32, 64)
    row = lax.broadcasted_iota(jnp.int32, shape, 0) + half_ref[0]
    diagonal = row == lax.broadcasted_iota(jnp.int32, shape, 1)

    def column(scale, factor):
        spread = jnp.where(diagonal, jnp.broadcast_to(scale[...], shape), 0.0)
        return jnp.sum(spread, axis=1, keepdims=True) * factor

    columns = {2: column(down_scale, 0.5), 5: column(out_scale, 1.0)}
    at = 0
    for k, (copy, buf) in enumerate(zip(copies, bufs)):
        copy.wait()
        value = buf[...].astype(BF)
        if k in columns:
            value = (value.astype(jnp.float32) * columns[k]).astype(BF)
        width = value.shape[1]
        for j in range(RING):
            out[j, :, at : at + width] = value
        at += width


def blocks(half, weights, scales):
    widths = [w.shape[1] for w in weights]
    vmem = pl.BlockSpec(memory_space=pltpu.VMEM)
    hbm = pl.BlockSpec(memory_space=pltpu.HBM)
    return pl.pallas_call(
        blocks_body,
        out_shape=jax.ShapeDtypeStruct((RING, 32, sum(widths)), BF),
        in_specs=[pl.BlockSpec(memory_space=pltpu.SMEM)] + [hbm] * 6 + [vmem] * 2,
        out_specs=vmem,
        scratch_shapes=[pltpu.VMEM((32, w), jnp.float32) for w in widths]
        + [pltpu.SemaphoreType.DMA((6,))],
    )(half[None], *weights, *[scale[None, :] for scale in scales])


def gather_chain(line):
    up, down = plane_shift(1), plane_shift(-1)
    forward, backward = line, line
    lines = [line]
    for step in range(1, 5):
        if step == 4:
            forward, backward = forward[:4], backward[4:]
        forward = lax.ppermute(forward, ALL, up)
        backward = lax.ppermute(backward, ALL, down)
        lines += [forward, backward]
    return lines


DELTAS = (0, -1, 1, -2, 2, -3, 3, -4, 4)


def silu(value):
    return value / (1.0 + jnp.exp(-value))


def matrix(ref, columns):
    value = ref[:, :, :, :, columns]
    return value.reshape(D, value.shape[-1])


def gated(normed, gate, up, gate_scale, up_scale):
    gate_part = jnp.dot(normed, gate, preferred_element_type=jnp.float32) * gate_scale[...]
    upward = jnp.dot(normed, up, preferred_element_type=jnp.float32) * up_scale[...]
    return (silu(gate_part) * upward).astype(BF)


def across(active, weight):
    return lax.dot_general(
        active, weight, (((1,), (1,)), ((), ())), preferred_element_type=jnp.float32
    ).astype(BF)


def normalize(rows, gain):
    values = rows.astype(jnp.float32)
    scaled = values * lax.rsqrt(jnp.mean(values * values, axis=-1, keepdims=True) + EPSILON)
    return (scaled * gain).astype(BF)


def line_copies(places, source, columns, dest, sem):
    copies = []
    for index, line in enumerate(source):
        p = places[index]
        for h in range(line.shape[0] // 4):
            half = h if line.shape[0] == 8 else (0 if index == 7 else 1)
            part = line.at[pl.ds(4 * h, 4), :, columns]
            copies.append(
                (
                    pltpu.make_async_copy(part, dest.at[:, p, half], sem),
                    pltpu.make_async_copy(part, dest.at[p % 4, pl.ds(4 * half, 4), p // 4], sem),
                )
            )
    return copies


def start_lines(core, groups):
    for which in range(2):

        @pl.when(core == which)
        def _():
            for group in groups:
                for pair in group:
                    pair[which].start()


def wait_lines(group):
    for copy, _ in group:
        copy.wait()


def own_and_other(core, count):
    own = pl.ds(pl.multiple_of(core * count, count), count)
    other = pl.ds(pl.multiple_of((1 - core) * count, count), count)
    return own, other


def entry_body(scalars, *refs):
    first, rest = refs[:9], refs[9:18]
    tokens, gain, gate_scale, up_scale = refs[18:22]
    sent, kept = refs[22:24]
    stored, placed = refs[24:29], refs[29:34]
    normed, sems = refs[34:]
    wide, down = placed[:2]
    core = scalars[0]
    places = [scalars[1 + k] for k in range(9)]
    ff = gate_scale.shape[1]
    everything = slice(None)
    groups = [line_copies(places, first, everything, wide, sems.at[0])]
    at = 0
    for k in range(1, 5):
        width = placed[k].shape[-1]
        groups.append(line_copies(places, rest, slice(at, at + width), placed[k], sems.at[k]))
        at += width
    start_lines(core, groups)
    stores = [
        pltpu.make_async_copy(src, dst, sems.at[5 + k])
        for k, (src, dst) in enumerate(zip(placed, stored))
    ]
    count = sent.shape[0]
    for at, rows in zip((0, count), own_and_other(core, count)):
        normed[at : at + count] = normalize(tokens[rows, :], gain[...])
    wait_lines(groups[0])
    stores[0].start()
    gate_part = jnp.dot(
        normed[...], matrix(wide, slice(0, ff)), preferred_element_type=jnp.float32
    ) * gate_scale[...]
    for group, store in zip(groups[1:], stores[1:]):
        wait_lines(group)
        store.start()
    upward = jnp.dot(
        normed[...], matrix(wide, slice(ff, 2 * ff)), preferred_element_type=jnp.float32
    ) * up_scale[...]
    hidden = (silu(gate_part) * upward).astype(BF)
    partial = across(hidden, matrix(down, everything))
    kept[...] = partial[:count]
    sent[...] = partial[count:]
    for store in stores:
        store.wait()


def entry(scalars, first, rest, tokens, gain, gate_scale, up_scale):
    rows = tokens.shape[0]
    ff = gate_scale.shape[0]
    smem = pl.BlockSpec(memory_space=pltpu.SMEM)
    hbm = pl.BlockSpec(memory_space=pltpu.HBM)
    vmem = pl.BlockSpec(memory_space=pltpu.VMEM)
    ch = (rest[0].shape[-1] - ff) // 3
    shapes = [(4, 8, 2, 32, width) for width in (2 * ff, ff, ch, ch, ch)]
    half = jax.ShapeDtypeStruct((rows // 2, D), BF)
    return pl.pallas_call(
        entry_body,
        out_shape=(half, half, *[jax.ShapeDtypeStruct(shape, BF) for shape in shapes]),
        in_specs=[smem] + [hbm] * 18 + [vmem] * 4,
        out_specs=(vmem, vmem, *[hbm] * 5),
        scratch_shapes=[pltpu.VMEM(shape, BF) for shape in shapes]
        + [pltpu.VMEM((rows, D), BF), pltpu.SemaphoreType.DMA((10,))],
        cost_estimate=pl.CostEstimate(
            flops=2 * rows * D * 3 * ff, bytes_accessed=16 << 20, transcendentals=rows * ff
        ),
    )(scalars, *first, *rest, tokens, gain[None, :], gate_scale[None, :], up_scale[None, :])


def again_body(own, other, wide, down, gate_scale, up_scale, sent, kept):
    rows = jnp.concatenate([own[...], other[...]], axis=0)
    ff = gate_scale.shape[1]
    hidden = gated(rows, wide[:, :ff], wide[:, ff:], gate_scale, up_scale)
    partial = across(hidden, down[...])
    count = own.shape[0]
    kept[...] = partial[:count]
    sent[...] = partial[count:]


def again(own, other, wide, down, gate_scale, up_scale):
    rows, ff = own.shape[0], gate_scale.shape[0]
    vmem = pl.BlockSpec(memory_space=pltpu.VMEM)
    half = jax.ShapeDtypeStruct((rows, D), BF)
    return pl.pallas_call(
        again_body,
        out_shape=(half, half),
        in_specs=[vmem] * 6,
        out_specs=(vmem, vmem),
        compiler_params=pltpu.CompilerParams(vmem_limit_bytes=24 << 20),
        cost_estimate=pl.CostEstimate(
            flops=2 * rows * D * 6 * ff, bytes_accessed=10 << 20, transcendentals=2 * rows * ff
        ),
    )(own, other, wide, down, gate_scale[None, :], up_scale[None, :])


def causal_depthwise(inputs, kernel):
    taps = kernel.shape[0]
    length = inputs.shape[0]
    padded = jnp.concatenate(
        [jnp.zeros((taps - 1, inputs.shape[1]), jnp.float32), inputs.astype(jnp.float32)], axis=0
    )
    total = jnp.zeros((length, inputs.shape[1]), jnp.float32)
    for offset in range(taps):
        total = total + kernel[offset] * padded[offset : offset + length]
    return total


def project(active, weight_rows):
    return lax.dot_general(
        active, weight_rows, (((1,), (1,)), ((), ())), preferred_element_type=jnp.float32
    ).astype(BF)


def rms_rows(rows, gains):
    values = rows.astype(jnp.float32)
    scaled = values * lax.rsqrt(jnp.mean(values * values, axis=-1, keepdims=True) + EPSILON)
    return (scaled * gains).astype(BF)


def sum_at_owner(own, other):
    pair = (own.astype(jnp.float32) + core_swap(other).astype(jnp.float32)).astype(BF)
    parts = over_x(pair.reshape(CHIPS, -1, D))
    return jnp.sum(parts.astype(jnp.float32), axis=0)


def collect(rows):
    own = over_x(jnp.broadcast_to(rows[None], (CHIPS, *rows.shape))).reshape(-1, D)
    return own, core_swap(own)


def local(
    tokens,
    gate_weight,
    up_weight,
    down_weight,
    value_weight,
    glu_weight,
    out_weight,
    gate_scale,
    up_scale,
    down_scale,
    value_scale,
    glu_scale,
    out_scale,
    conv_kernel,
    norm_gain,
    first_gain,
    conv_gain,
    second_gain,
):
    rep, fs, tp = lax.axis_index("rep"), lax.axis_index("fs"), lax.axis_index("tp")
    core, chip = tp % 2, tp // 2
    ring_z, ring_y = rep * 4 + fs // 8, fs % 8
    first_core = core == 0
    me = jnp.where(first_core, ring_y, ring_z)

    scalars = jnp.stack([core] + [(me + delta + RING) % RING for delta in DELTAS])
    block = blocks(
        rep * 32,
        (gate_weight, up_weight, down_weight, value_weight, glu_weight, out_weight),
        (down_scale, out_scale),
    )
    line = lax.all_to_all(block, ALL, 0, 0, axis_index_groups=plane_groups(), tiled=True)
    ff = gate_weight.shape[1]
    ch = value_weight.shape[1]
    first = gather_chain(line[:, :, : 2 * ff])
    rest = gather_chain(line[:, :, 2 * ff :])
    rows_half = tokens.shape[0] // 2
    own_count = rows_half // CHIPS
    sent, mine, *placed = entry(scalars, first, rest, tokens, first_gain, gate_scale, up_scale)
    wide, down, value_full, glu_full, out_full = [p.reshape(D, p.shape[-1]) for p in placed]

    def halves(full):
        own = lax.dynamic_slice_in_dim(full, core * rows_half, rows_half, 0)
        other = lax.dynamic_slice_in_dim(full, (1 - core) * rows_half, rows_half, 0)
        return own, other

    def in_order(own, other):
        return jnp.concatenate(
            [jnp.where(first_core, own, other), jnp.where(first_core, other, own)], axis=0
        )

    own_tokens = lax.dynamic_slice_in_dim(
        tokens, core * rows_half + chip * own_count, own_count, 0
    )
    after_first = (own_tokens.astype(jnp.float32) + sum_at_owner(mine, sent)).astype(BF)

    def glu_of(rows):
        value_part = jnp.dot(rows, value_full, preferred_element_type=jnp.float32) * value_scale
        gate_part = jnp.dot(rows, glu_full, preferred_element_type=jnp.float32) * glu_scale
        return (value_part * jax.nn.sigmoid(gate_part)).astype(BF)

    own, other = collect(rms_rows(after_first, conv_gain))
    mixed = causal_depthwise(in_order(glu_of(own), glu_of(other)), conv_kernel)
    stats = jnp.stack([jnp.sum(mixed, axis=1), jnp.sum(mixed * mixed, axis=1)])
    stats = lax.all_to_all(jnp.broadcast_to(stats[None], (8, *stats.shape)), "tp", 0, 0, tiled=True)
    stats = jnp.sum(stats, axis=0) / D
    mean_rows, square_rows = stats[0][:, None], stats[1][:, None]
    normalized = (
        (mixed - mean_rows) * lax.rsqrt(square_rows - mean_rows * mean_rows + EPSILON) * norm_gain
    )
    active = jax.nn.silu(normalized).astype(BF)
    after_conv = (
        after_first.astype(jnp.float32) + sum_at_owner(*halves(project(active, out_full)))
    ).astype(BF)

    own, other = collect(rms_rows(after_conv, second_gain))
    sent, mine = again(own, other, wide, down, gate_scale, up_scale)
    total = sum_at_owner(mine, sent)
    after_second = (after_conv.astype(jnp.float32) + total).astype(BF)
    return in_order(*collect(after_second))


def solution(mesh):
    placed = (
        P(("rep", "fs"), None),
        P("fs", "tp"),
        P("fs", "tp"),
        P("fs", "tp"),
        P("fs", "tp"),
        P("fs", "tp"),
        P("fs", "tp"),
        P("tp"),
        P("tp"),
        P("fs"),
        P("tp"),
        P("tp"),
        P("fs"),
        P(None, "tp"),
        P("tp"),
        P(),
        P(),
        P(),
    )
    return jax.shard_map(
        local, mesh=mesh, in_specs=placed, out_specs=P(("rep", "fs"), None), check_vma=False
    )
```

```python
import jax
import jax.numpy as jnp
from jax import lax
from jax.experimental import pallas as pl
from jax.experimental.pallas import tpu as pltpu
from jax.sharding import PartitionSpec as P


D = 2048
EPSILON = 1e-06
RING = 8
CHIPS = 4
ALL = ("rep", "fs", "tp")
BF = jnp.bfloat16


def device_id(ring_z, y, x, core):
    return (ring_z // 4) * 256 + ((ring_z % 4) * 8 + y) * 8 + x * 2 + core


def plane_groups():
    groups = []
    for x in range(CHIPS):
        for p in range(RING):
            groups.append([device_id(z, p, x, 0) for z in range(RING)])
            groups.append([device_id(p, y, x, 1) for y in range(RING)])
    return groups


def plane_shift(step):
    pairs = []
    for x in range(CHIPS):
        for z in range(RING):
            for y in range(RING):
                pairs.append((device_id(z, y, x, 0), device_id(z, (y + step) % RING, x, 0)))
                pairs.append((device_id(z, y, x, 1), device_id((z + step) % RING, y, x, 1)))
    return pairs


def core_swap(value):
    return lax.ppermute(value, "tp", [(i, i ^ 1) for i in range(8)])


def over_x(value):
    groups = [[0, 2, 4, 6], [1, 3, 5, 7]]
    return lax.all_to_all(value, "tp", 0, 0, axis_index_groups=groups, tiled=True)


def blocks_body(*refs):
    weights, (down_scale, out_scale, out), bufs, sem = refs[:6], refs[6:9], refs[9:15], refs[15]
    start = pl.multiple_of(lax.axis_index("rep") * 32, 32)
    copies = [
        pltpu.make_async_copy(w.at[pl.ds(start, 32)], buf, sem.at[k])
        for k, (w, buf) in enumerate(zip(weights, bufs))
    ]
    for copy in copies:
        copy.start()
    shape = (32, 64)
    index = lax.broadcasted_iota(jnp.int32, shape, 0) + start
    diagonal = index == lax.broadcasted_iota(jnp.int32, shape, 1)

    def column(scale, factor):
        spread = jnp.where(diagonal, jnp.broadcast_to(row(scale), shape), 0.0)
        return jnp.sum(spread, axis=1, keepdims=True) * factor

    columns = {2: column(down_scale, 0.5), 5: column(out_scale, 1.0)}
    at = 0
    for k, (copy, buf) in enumerate(zip(copies, bufs)):
        copy.wait()
        value = buf[...].astype(BF)
        if k in columns:
            value = (value.astype(jnp.float32) * columns[k]).astype(BF)
        width = value.shape[1]
        for j in range(RING):
            out[j, :, at : at + width] = value
        at += width


def blocks(weights, scales):
    widths = [w.shape[1] for w in weights]
    vmem = pl.BlockSpec(memory_space=pltpu.VMEM)
    hbm = pl.BlockSpec(memory_space=pltpu.HBM)
    return pl.pallas_call(
        blocks_body,
        out_shape=jax.ShapeDtypeStruct((RING, 32, sum(widths)), BF),
        in_specs=[hbm] * 6 + [vmem] * 2,
        out_specs=vmem,
        scratch_shapes=[pltpu.VMEM((32, w), jnp.float32) for w in widths]
        + [pltpu.SemaphoreType.DMA((6,))],
    )(*weights, *scales)


def gather_lines(line):
    up, down = plane_shift(1), plane_shift(-1)
    parts = [line[: RING // 2], line[RING // 2 :]]
    moving = [[part, part] for part in parts]
    chains = [[part] for part in parts]
    for step in range(1, 5):
        for k in range(2):
            for way, shift in enumerate((up, down)):
                if step < 4 or way != k:
                    moving[k][way] = lax.ppermute(moving[k][way], ALL, shift)
                    chains[k].append(moving[k][way])
    return chains


DELTAS = (0, -1, 1, -2, 2, -3, 3, 4)


def position():
    rep, fs, tp = lax.axis_index("rep"), lax.axis_index("fs"), lax.axis_index("tp")
    core, chip = lax.rem(tp, 2), lax.div(tp, 2)
    ring_z, ring_y = rep * 4 + lax.div(fs, RING), lax.rem(fs, RING)
    return rep, core, chip, jnp.where(core == 0, ring_y, ring_z)


def silu(value):
    return value / (1.0 + jnp.exp(-value))


def matrix(ref, columns):
    value = ref[:, :, :, :, columns]
    return value.reshape(D, value.shape[-1])


def row(ref):
    return ref[...].reshape(1, -1)


def gated(normed, gate, up, gate_scale, up_scale):
    gate_part = jnp.dot(normed, gate, preferred_element_type=jnp.float32) * row(gate_scale)
    upward = jnp.dot(normed, up, preferred_element_type=jnp.float32) * row(up_scale)
    return (silu(gate_part) * upward).astype(BF)


def across(active, weight):
    return lax.dot_general(
        active, weight, (((1,), (1,)), ((), ())), preferred_element_type=jnp.float32
    ).astype(BF)


def normalize(rows, gain):
    values = rows.astype(jnp.float32)
    scaled = values * lax.rsqrt(jnp.mean(values * values, axis=-1, keepdims=True) + EPSILON)
    return (scaled * gain).astype(BF)


def line_copies(me, source, half, dest, sem):
    columns = slice(0, dest.shape[-1])
    copies = []
    for delta, line in zip(DELTAS, source):
        p = lax.rem(me + (delta + RING), RING)
        z_low, rep = lax.rem(p, 4), lax.div(p, 4)
        part = line.at[:, :, columns]
        copies.append(
            (
                pltpu.make_async_copy(part, dest.at[:, p, half], sem),
                pltpu.make_async_copy(part, dest.at[z_low, pl.ds(4 * half, 4), rep], sem),
            )
        )
    return copies


def start_lines(core, groups):
    for which in range(2):

        @pl.when(core == which)
        def _():
            for group in groups:
                for pair in group:
                    pair[which].start()


def wait_lines(group):
    for copy, _ in group:
        copy.wait()


def own_and_other(core, count):
    own = pl.ds(pl.multiple_of(core * count, count), count)
    other = pl.ds(pl.multiple_of((1 - core) * count, count), count)
    return own, other


def entry_body(*refs):
    chains = refs[:8], refs[8:16]
    tokens, gain, gate_scale, up_scale = refs[16:20]
    sent, kept, own_tokens = refs[20:23]
    stored = refs[23:26]
    placed, normed, sems = refs[26:]
    ff = gate_scale.shape[0]
    _, core, chip, me = position()
    groups = [line_copies(me, chain, k, placed, sems.at[k]) for k, chain in enumerate(chains)]
    start_lines(core, groups)
    stores, at = [], 3 * ff
    for k, out in enumerate(stored):
        width = out.shape[-1]
        part = placed.at[:, :, :, :, at : at + width]
        stores.append(pltpu.make_async_copy(part, out, sems.at[2 + k]))
        at += width
    count, size = sent.shape[0], own_tokens.shape[0]
    for at, rows in zip((0, count), own_and_other(core, count)):
        normed[at : at + count] = normalize(tokens[rows, :], row(gain))
    own_tokens[...] = tokens[pl.ds(pl.multiple_of(core * count + chip * size, 8), size), :]
    for group in groups:
        wait_lines(group)
    for store in stores:
        store.start()
    gate, up, down = [matrix(placed, slice(k * ff, (k + 1) * ff)) for k in range(3)]
    hidden = gated(normed[...], gate, up, gate_scale, up_scale)
    partial = across(hidden, down)
    kept[...] = partial[:count]
    sent[...] = partial[count:]
    for store in stores:
        store.wait()


def entry(chains, tokens, gain, gate_scale, up_scale):
    rows = tokens.shape[0]
    ff = gate_scale.shape[0]
    hbm = pl.BlockSpec(memory_space=pltpu.HBM)
    vmem = pl.BlockSpec(memory_space=pltpu.VMEM)
    total = chains[0][0].shape[-1]
    ch = (total - 3 * ff) // 3
    half = jax.ShapeDtypeStruct((rows // 2, D), BF)
    own = jax.ShapeDtypeStruct((rows // 8, D), BF)
    shape = (4, RING, 2, 32)
    weights = [jax.ShapeDtypeStruct((*shape, w), BF) for w in (ch, ch, ch)]
    return pl.pallas_call(
        entry_body,
        out_shape=(half, half, own, *weights),
        in_specs=[hbm] * 16 + [vmem] * 4,
        out_specs=(vmem, vmem, vmem, hbm, hbm, hbm),
        scratch_shapes=[
            pltpu.VMEM((*shape, total), BF),
            pltpu.VMEM((rows, D), BF),
            pltpu.SemaphoreType.DMA((5,)),
        ],
        cost_estimate=pl.CostEstimate(
            flops=2 * rows * D * 3 * ff, bytes_accessed=24 << 20, transcendentals=rows * ff
        ),
    )(*chains[0], *chains[1], tokens, gain, gate_scale, up_scale)


def again_body(*refs):
    chains = refs[:8], refs[8:16]
    own, other, gate_scale, up_scale, sent, kept, placed, sems = refs[16:]
    _, core, _, me = position()
    groups = [line_copies(me, chain, k, placed, sems.at[k]) for k, chain in enumerate(chains)]
    start_lines(core, groups)
    ff = gate_scale.shape[0]
    rows = jnp.concatenate([own[...], other[...]], axis=0)
    for group in groups:
        wait_lines(group)
    gate, up, down = [matrix(placed, slice(k * ff, (k + 1) * ff)) for k in range(3)]
    partial = across(gated(rows, gate, up, gate_scale, up_scale), down)
    count = own.shape[0]
    kept[...] = partial[:count]
    sent[...] = partial[count:]


def again(chains, own, other, gate_scale, up_scale):
    rows, ff = own.shape[0], gate_scale.shape[0]
    hbm = pl.BlockSpec(memory_space=pltpu.HBM)
    vmem = pl.BlockSpec(memory_space=pltpu.VMEM)
    half = jax.ShapeDtypeStruct((rows, D), BF)
    return pl.pallas_call(
        again_body,
        out_shape=(half, half),
        in_specs=[hbm] * 16 + [vmem] * 4,
        out_specs=(vmem, vmem),
        scratch_shapes=[
            pltpu.VMEM((4, RING, 2, 32, 3 * ff), BF),
            pltpu.SemaphoreType.DMA((2,)),
        ],
        compiler_params=pltpu.CompilerParams(vmem_limit_bytes=32 << 20),
        cost_estimate=pl.CostEstimate(
            flops=2 * rows * D * 6 * ff, bytes_accessed=10 << 20, transcendentals=2 * rows * ff
        ),
    )(*chains[0], *chains[1], own, other, gate_scale, up_scale)


def causal_depthwise(inputs, kernel):
    taps = kernel.shape[0]
    length = inputs.shape[0]
    padded = jnp.concatenate(
        [jnp.zeros((taps - 1, inputs.shape[1]), jnp.float32), inputs.astype(jnp.float32)], axis=0
    )
    total = jnp.zeros((length, inputs.shape[1]), jnp.float32)
    for offset in range(taps):
        total = total + kernel[offset] * padded[offset : offset + length]
    return total


def project(active, weight_rows):
    return lax.dot_general(
        active, weight_rows, (((1,), (1,)), ((), ())), preferred_element_type=jnp.float32
    ).astype(BF)


def rms_rows(rows, gains):
    values = rows.astype(jnp.float32)
    scaled = values * lax.rsqrt(jnp.mean(values * values, axis=-1, keepdims=True) + EPSILON)
    return (scaled * gains).astype(BF)


def sum_at_owner(own, other):
    pair = (own.astype(jnp.float32) + core_swap(other).astype(jnp.float32)).astype(BF)
    parts = over_x(pair.reshape(CHIPS, -1, D))
    return jnp.sum(parts.astype(jnp.float32), axis=0)


def collect(rows):
    own = over_x(jnp.broadcast_to(rows[None], (CHIPS, *rows.shape))).reshape(-1, D)
    return own, core_swap(own)


def local(
    tokens,
    gate_weight,
    up_weight,
    down_weight,
    value_weight,
    glu_weight,
    out_weight,
    gate_scale,
    up_scale,
    down_scale,
    value_scale,
    glu_scale,
    out_scale,
    conv_kernel,
    norm_gain,
    first_gain,
    conv_gain,
    second_gain,
):
    _, core, _, _ = position()
    first_core = core == 0
    block = blocks(
        (gate_weight, up_weight, down_weight, value_weight, glu_weight, out_weight),
        (down_scale, out_scale),
    )
    line = lax.all_to_all(block, ALL, 0, 0, axis_index_groups=plane_groups(), tiled=True)
    rows_half = tokens.shape[0] // 2
    chains = gather_lines(line)
    sent, mine, own_tokens, *placed = entry(chains, tokens, first_gain, gate_scale, up_scale)
    value_full, glu_full, out_full = [p.reshape(D, p.shape[-1]) for p in placed]

    def halves(full):
        low, high = full[:rows_half], full[rows_half:]
        return jnp.where(first_core, low, high), jnp.where(first_core, high, low)

    def in_order(own, other):
        return jnp.concatenate(
            [jnp.where(first_core, own, other), jnp.where(first_core, other, own)], axis=0
        )

    after_first = (own_tokens.astype(jnp.float32) + sum_at_owner(mine, sent)).astype(BF)

    def glu_of(rows):
        value_part = jnp.dot(rows, value_full, preferred_element_type=jnp.float32) * value_scale
        gate_part = jnp.dot(rows, glu_full, preferred_element_type=jnp.float32) * glu_scale
        return (value_part * jax.nn.sigmoid(gate_part)).astype(BF)

    own, other = collect(rms_rows(after_first, conv_gain))
    mixed = causal_depthwise(in_order(glu_of(own), glu_of(other)), conv_kernel)
    stats = jnp.stack([jnp.sum(mixed, axis=1), jnp.sum(mixed * mixed, axis=1)])
    stats = lax.all_to_all(jnp.broadcast_to(stats[None], (8, *stats.shape)), "tp", 0, 0, tiled=True)
    stats = jnp.sum(stats, axis=0) / D
    mean_rows, square_rows = stats[0][:, None], stats[1][:, None]
    normalized = (
        (mixed - mean_rows) * lax.rsqrt(square_rows - mean_rows * mean_rows + EPSILON) * norm_gain
    )
    active = jax.nn.silu(normalized).astype(BF)
    after_conv = (
        after_first.astype(jnp.float32) + sum_at_owner(*halves(project(active, out_full)))
    ).astype(BF)

    own, other = collect(rms_rows(after_conv, second_gain))
    sent, mine = again(chains, own, other, gate_scale, up_scale)
    total = sum_at_owner(mine, sent)
    after_second = (after_conv.astype(jnp.float32) + total).astype(BF)
    return in_order(*collect(after_second))


def solution(mesh):
    placed = (
        P(("rep", "fs"), None),
        P("fs", "tp"),
        P("fs", "tp"),
        P("fs", "tp"),
        P("fs", "tp"),
        P("fs", "tp"),
        P("fs", "tp"),
        P("tp"),
        P("tp"),
        P("fs"),
        P("tp"),
        P("tp"),
        P("fs"),
        P(None, "tp"),
        P("tp"),
        P(),
        P(),
        P(),
    )
    return jax.shard_map(
        local, mesh=mesh, in_specs=placed, out_specs=P(("rep", "fs"), None), check_vma=False
    )
```

```python
import jax
import jax.numpy as jnp
from jax import lax
from jax.experimental import pallas as pl
from jax.experimental.pallas import tpu as pltpu
from jax.sharding import PartitionSpec as P


D = 2048
EPSILON = 1e-06
RING = 8
CHIPS = 4
ALL = ("rep", "fs", "tp")
BF = jnp.bfloat16


def device_id(ring_z, y, x, core):
    return (ring_z // 4) * 256 + ((ring_z % 4) * 8 + y) * 8 + x * 2 + core


def plane_groups():
    groups = []
    for x in range(CHIPS):
        for p in range(RING):
            groups.append([device_id(z, p, x, 0) for z in range(RING)])
            groups.append([device_id(p, y, x, 1) for y in range(RING)])
    return groups


def plane_shift(step):
    pairs = []
    for x in range(CHIPS):
        for z in range(RING):
            for y in range(RING):
                pairs.append((device_id(z, y, x, 0), device_id(z, (y + step) % RING, x, 0)))
                pairs.append((device_id(z, y, x, 1), device_id((z + step) % RING, y, x, 1)))
    return pairs


def core_swap(value):
    return lax.ppermute(value, "tp", [(i, i ^ 1) for i in range(8)])


def over_x(value):
    groups = [[0, 2, 4, 6], [1, 3, 5, 7]]
    return lax.all_to_all(value, "tp", 0, 0, axis_index_groups=groups, tiled=True)


def blocks_body(*refs):
    weights, (down_scale, out_scale, out), bufs, sem = refs[:6], refs[6:9], refs[9:15], refs[15]
    start = pl.multiple_of(lax.axis_index("rep") * 32, 32)
    copies = [
        pltpu.make_async_copy(w.at[pl.ds(start, 32)], buf, sem.at[k])
        for k, (w, buf) in enumerate(zip(weights, bufs))
    ]
    for copy in copies:
        copy.start()
    shape = (32, 64)
    index = lax.broadcasted_iota(jnp.int32, shape, 0) + start
    diagonal = index == lax.broadcasted_iota(jnp.int32, shape, 1)

    def column(scale, factor):
        spread = jnp.where(diagonal, jnp.broadcast_to(row(scale), shape), 0.0)
        return jnp.sum(spread, axis=1, keepdims=True) * factor

    columns = {2: column(down_scale, 0.5), 5: column(out_scale, 1.0)}
    at = 0
    for k, (copy, buf) in enumerate(zip(copies, bufs)):
        copy.wait()
        value = buf[...].astype(BF)
        if k in columns:
            value = (value.astype(jnp.float32) * columns[k]).astype(BF)
        width = value.shape[1]
        for j in range(RING):
            out[j, :, at : at + width] = value
        at += width


def blocks(weights, scales):
    widths = [w.shape[1] for w in weights]
    vmem = pl.BlockSpec(memory_space=pltpu.VMEM)
    hbm = pl.BlockSpec(memory_space=pltpu.HBM)
    return pl.pallas_call(
        blocks_body,
        out_shape=jax.ShapeDtypeStruct((RING, 32, sum(widths)), BF),
        in_specs=[hbm] * 6 + [vmem] * 2,
        out_specs=vmem,
        scratch_shapes=[pltpu.VMEM((32, w), jnp.float32) for w in widths]
        + [pltpu.SemaphoreType.DMA((6,))],
    )(*weights, *scales)


def gather_lines(line):
    up, down = plane_shift(1), plane_shift(-1)
    parts = [line[: RING // 2], line[RING // 2 :]]
    moving = [[part, part] for part in parts]
    chains = [[part] for part in parts]
    for step in range(1, 5):
        for k in range(2):
            for way, shift in enumerate((up, down)):
                if step < 4 or way != k:
                    moving[k][way] = lax.ppermute(moving[k][way], ALL, shift)
                    chains[k].append(moving[k][way])
    return chains


DELTAS = (0, -1, 1, -2, 2, -3, 3, 4)


def position():
    rep, fs, tp = lax.axis_index("rep"), lax.axis_index("fs"), lax.axis_index("tp")
    core, chip = lax.rem(tp, 2), lax.div(tp, 2)
    ring_z, ring_y = rep * 4 + lax.div(fs, RING), lax.rem(fs, RING)
    return rep, core, chip, jnp.where(core == 0, ring_y, ring_z)


def silu(value):
    return value / (1.0 + jnp.exp(-value))


def matrix(ref, columns):
    value = ref[:, :, :, :, columns]
    return value.reshape(D, value.shape[-1])


def row(ref):
    return ref[...].reshape(1, -1)


def gated(normed, gate, up, gate_scale, up_scale):
    gate_part = jnp.dot(normed, gate, preferred_element_type=jnp.float32) * row(gate_scale)
    upward = jnp.dot(normed, up, preferred_element_type=jnp.float32) * row(up_scale)
    return (silu(gate_part) * upward).astype(BF)


def across(active, weight):
    return lax.dot_general(
        active, weight, (((1,), (1,)), ((), ())), preferred_element_type=jnp.float32
    ).astype(BF)


def normalize(rows, gain):
    values = rows.astype(jnp.float32)
    scaled = values * lax.rsqrt(jnp.mean(values * values, axis=-1, keepdims=True) + EPSILON)
    return (scaled * gain).astype(BF)


def line_copies(me, source, half, dest, sem):
    columns = slice(0, dest.shape[-1])
    copies = []
    for delta, line in zip(DELTAS, source):
        p = lax.rem(me + (delta + RING), RING)
        z_low, rep = lax.rem(p, 4), lax.div(p, 4)
        part = line.at[:, :, columns]
        copies.append(
            (
                pltpu.make_async_copy(part, dest.at[:, p, half], sem),
                pltpu.make_async_copy(part, dest.at[z_low, pl.ds(4 * half, 4), rep], sem),
            )
        )
    return copies


def start_lines(core, groups):
    for which in range(2):

        @pl.when(core == which)
        def _():
            for group in groups:
                for pair in group:
                    pair[which].start()


def wait_lines(group):
    for copy, _ in group:
        copy.wait()


def own_and_other(core, count):
    own = pl.ds(pl.multiple_of(core * count, count), count)
    other = pl.ds(pl.multiple_of((1 - core) * count, count), count)
    return own, other


def entry_body(flag, *refs):
    chains = refs[:8], refs[8:16]
    tokens, gain, gate_scale, up_scale = refs[16:20]
    sent, kept, own_tokens = refs[20:23]
    stored = refs[23:26]
    placed, normed, sems = refs[26:]
    ff = gate_scale.shape[0]
    _, _, chip, me = position()
    core = flag[0]
    groups = [line_copies(me, chain, k, placed, sems.at[k]) for k, chain in enumerate(chains)]
    start_lines(core, groups)
    stores, at = [], 3 * ff
    for k, out in enumerate(stored):
        width = out.shape[-1]
        part = placed.at[:, :, :, :, at : at + width]
        stores.append(pltpu.make_async_copy(part, out, sems.at[2 + k]))
        at += width
    count, size = sent.shape[0], own_tokens.shape[0]
    for at, rows in zip((0, count), own_and_other(core, count)):
        normed[at : at + count] = normalize(tokens[rows, :], row(gain))
    own_tokens[...] = tokens[pl.ds(pl.multiple_of(core * count + chip * size, 8), size), :]
    for group in groups:
        wait_lines(group)
    for store in stores:
        store.start()
    gate, up, down = [matrix(placed, slice(k * ff, (k + 1) * ff)) for k in range(3)]
    hidden = gated(normed[...], gate, up, gate_scale, up_scale)
    partial = across(hidden, down)
    kept[...] = partial[:count]
    sent[...] = partial[count:]
    for store in stores:
        store.wait()


def entry(flag, chains, tokens, gain, gate_scale, up_scale):
    rows = tokens.shape[0]
    ff = gate_scale.shape[0]
    hbm = pl.BlockSpec(memory_space=pltpu.HBM)
    vmem = pl.BlockSpec(memory_space=pltpu.VMEM)
    total = chains[0][0].shape[-1]
    ch = (total - 3 * ff) // 3
    half = jax.ShapeDtypeStruct((rows // 2, D), BF)
    own = jax.ShapeDtypeStruct((rows // 8, D), BF)
    shape = (4, RING, 2, 32)
    weights = [jax.ShapeDtypeStruct((*shape, w), BF) for w in (ch, ch, ch)]
    return pl.pallas_call(
        entry_body,
        out_shape=(half, half, own, *weights),
        in_specs=[pl.BlockSpec(memory_space=pltpu.SMEM)] + [hbm] * 16 + [vmem] * 4,
        out_specs=(vmem, vmem, vmem, hbm, hbm, hbm),
        scratch_shapes=[
            pltpu.VMEM((*shape, total), BF),
            pltpu.VMEM((rows, D), BF),
            pltpu.SemaphoreType.DMA((5,)),
        ],
        compiler_params=pltpu.CompilerParams(vmem_limit_bytes=48 << 20),
        cost_estimate=pl.CostEstimate(
            flops=2 * rows * D * 3 * ff, bytes_accessed=24 << 20, transcendentals=rows * ff
        ),
    )(flag[None], *chains[0], *chains[1], tokens, gain, gate_scale, up_scale)


def again_body(*refs):
    chains = refs[:8], refs[8:16]
    own, other, gate_scale, up_scale, sent, kept, placed, sems = refs[16:]
    _, core, _, me = position()
    groups = [line_copies(me, chain, k, placed, sems.at[k]) for k, chain in enumerate(chains)]
    start_lines(core, groups)
    ff = gate_scale.shape[0]
    rows = jnp.concatenate([own[...], other[...]], axis=0)
    for group in groups:
        wait_lines(group)
    gate, up, down = [matrix(placed, slice(k * ff, (k + 1) * ff)) for k in range(3)]
    partial = across(gated(rows, gate, up, gate_scale, up_scale), down)
    count = own.shape[0]
    kept[...] = partial[:count]
    sent[...] = partial[count:]


def again(chains, own, other, gate_scale, up_scale):
    rows, ff = own.shape[0], gate_scale.shape[0]
    hbm = pl.BlockSpec(memory_space=pltpu.HBM)
    vmem = pl.BlockSpec(memory_space=pltpu.VMEM)
    half = jax.ShapeDtypeStruct((rows, D), BF)
    return pl.pallas_call(
        again_body,
        out_shape=(half, half),
        in_specs=[hbm] * 16 + [vmem] * 4,
        out_specs=(vmem, vmem),
        scratch_shapes=[
            pltpu.VMEM((4, RING, 2, 32, 3 * ff), BF),
            pltpu.SemaphoreType.DMA((2,)),
        ],
        compiler_params=pltpu.CompilerParams(vmem_limit_bytes=32 << 20),
        cost_estimate=pl.CostEstimate(
            flops=2 * rows * D * 6 * ff, bytes_accessed=10 << 20, transcendentals=2 * rows * ff
        ),
    )(*chains[0], *chains[1], own, other, gate_scale, up_scale)


def causal_depthwise(inputs, kernel):
    taps = kernel.shape[0]
    length = inputs.shape[0]
    padded = jnp.concatenate(
        [jnp.zeros((taps - 1, inputs.shape[1]), jnp.float32), inputs.astype(jnp.float32)], axis=0
    )
    total = jnp.zeros((length, inputs.shape[1]), jnp.float32)
    for offset in range(taps):
        total = total + kernel[offset] * padded[offset : offset + length]
    return total


def project(active, weight_rows):
    return lax.dot_general(
        active, weight_rows, (((1,), (1,)), ((), ())), preferred_element_type=jnp.float32
    ).astype(BF)


def rms_rows(rows, gains):
    values = rows.astype(jnp.float32)
    scaled = values * lax.rsqrt(jnp.mean(values * values, axis=-1, keepdims=True) + EPSILON)
    return (scaled * gains).astype(BF)


def sum_at_owner(own, other):
    pair = (own.astype(jnp.float32) + core_swap(other).astype(jnp.float32)).astype(BF)
    parts = over_x(pair.reshape(CHIPS, -1, D))
    return jnp.sum(parts.astype(jnp.float32), axis=0)


def collect(rows):
    own = over_x(jnp.broadcast_to(rows[None], (CHIPS, *rows.shape))).reshape(-1, D)
    return own, core_swap(own)


def local(
    tokens,
    gate_weight,
    up_weight,
    down_weight,
    value_weight,
    glu_weight,
    out_weight,
    gate_scale,
    up_scale,
    down_scale,
    value_scale,
    glu_scale,
    out_scale,
    conv_kernel,
    norm_gain,
    first_gain,
    conv_gain,
    second_gain,
):
    _, core, _, _ = position()
    first_core = core == 0
    flag = jnp.where(first_core, 0, 1)
    block = blocks(
        (gate_weight, up_weight, down_weight, value_weight, glu_weight, out_weight),
        (down_scale, out_scale),
    )
    line = lax.all_to_all(block, ALL, 0, 0, axis_index_groups=plane_groups(), tiled=True)
    rows_half = tokens.shape[0] // 2
    chains = gather_lines(line)
    sent, mine, own_tokens, *placed = entry(
        flag, chains, tokens, first_gain, gate_scale, up_scale
    )
    value_full, glu_full, out_full = [p.reshape(D, p.shape[-1]) for p in placed]

    def halves(full):
        low, high = full[:rows_half], full[rows_half:]
        return jnp.where(first_core, low, high), jnp.where(first_core, high, low)

    def in_order(own, other):
        return jnp.concatenate(
            [jnp.where(first_core, own, other), jnp.where(first_core, other, own)], axis=0
        )

    after_first = (own_tokens.astype(jnp.float32) + sum_at_owner(mine, sent)).astype(BF)

    def glu_of(rows):
        value_part = jnp.dot(rows, value_full, preferred_element_type=jnp.float32) * value_scale
        gate_part = jnp.dot(rows, glu_full, preferred_element_type=jnp.float32) * glu_scale
        return (value_part * jax.nn.sigmoid(gate_part)).astype(BF)

    own, other = collect(rms_rows(after_first, conv_gain))
    mixed = causal_depthwise(in_order(glu_of(own), glu_of(other)), conv_kernel)
    stats = jnp.stack([jnp.sum(mixed, axis=1), jnp.sum(mixed * mixed, axis=1)])
    stats = lax.all_to_all(jnp.broadcast_to(stats[None], (8, *stats.shape)), "tp", 0, 0, tiled=True)
    stats = jnp.sum(stats, axis=0) / D
    mean_rows, square_rows = stats[0][:, None], stats[1][:, None]
    normalized = (
        (mixed - mean_rows) * lax.rsqrt(square_rows - mean_rows * mean_rows + EPSILON) * norm_gain
    )
    active = jax.nn.silu(normalized).astype(BF)
    after_conv = (
        after_first.astype(jnp.float32) + sum_at_owner(*halves(project(active, out_full)))
    ).astype(BF)

    own, other = collect(rms_rows(after_conv, second_gain))
    sent, mine = again(chains, own, other, gate_scale, up_scale)
    total = sum_at_owner(mine, sent)
    after_second = (after_conv.astype(jnp.float32) + total).astype(BF)
    return in_order(*collect(after_second))


def solution(mesh):
    placed = (
        P(("rep", "fs"), None),
        P("fs", "tp"),
        P("fs", "tp"),
        P("fs", "tp"),
        P("fs", "tp"),
        P("fs", "tp"),
        P("fs", "tp"),
        P("tp"),
        P("tp"),
        P("fs"),
        P("tp"),
        P("tp"),
        P("fs"),
        P(None, "tp"),
        P("tp"),
        P(),
        P(),
        P(),
    )
    return jax.shard_map(
        local, mesh=mesh, in_specs=placed, out_specs=P(("rep", "fs"), None), check_vma=False
    )
```
